256 devices in a mesh: sp: 64 (over z, y, core), tp: 4 (over x).
Axes of the slice: x: 4, y: 4, z: 8, core: 2. Of those that a mesh axis runs over, the one named last changes fastest.
Arguments:
- pooled_in: bfloat16 [65536, 2048], P('sp', 'tp'), may hold values from -6 to 6
- group_map: bfloat16 [4, 512, 512], P('tp'), may hold values from -0.25 to 0.25
- pool_scale: float32 [2048], P('tp'), may hold values from 0.1 to 1.9
- out_weight: bfloat16 [2048, 2048], P('tp'), may hold values from -0.125 to 0.125
- residual: bfloat16 [65536, 2048], P(('sp', 'tp')), may hold values from -6 to 6
- norm_gain: float32 [2048], replicated, may hold values from 0.1 to 1.9
- gate_weight: bfloat16 [64, 2048, 512], P('sp'), may hold values from -0.125 to 0.125
- up_weight: bfloat16 [64, 2048, 512], P('sp'), may hold values from -0.125 to 0.125
- down_weight: bfloat16 [64, 512, 2048], P('sp'), may hold values from -0.25 to 0.25
- route_expert: int32 [65536, 2], P(('sp', 'tp')), may hold values from 0 to 63, all different within a row; in each aligned block of 256 rows (0 to 255, 256 to 511, ...) at most 12 rows name the same one
- route_score: float32 [65536, 2], P(('sp', 'tp')), may hold values from 0.05 to 1
Outputs:
- layer_out: bfloat16 [65536, 2048], P(('sp', 'tp'))
The draws below stay inside these ranges and needn't reach their ends.
Inputs may be any that keep to these rules, and one draw needn't show every extreme that they name: `route_expert`: each token names 2 different experts. Within each aligned block of 256 tokens (the rows of one device) no expert is named by more than 12 tokens, and in some such block one expert is named by exactly 12.
All inputs are finite; a program needn't handle non-finite values.
Results may differ from the reference program's by a relative error of at most 0.0065.
Values may be sent and summed in bfloat16 or wider, within the bound.
A program may use at most 64 MiB of HBM per device.

```python
import math
import jax
import jax.numpy as jnp
import numpy as np
from jax import lax

D = 2048
GROUPS = 4
D_POOL = 2048
GROUP = 512
FF = 512
TOP = 2
ROWS_DEV = 256
TOKENS = 65536
EXPERTS = 64
CAP = 12


def block_scale(own_key, shape, split, least, largest):
    gain = 1.0
    for axis_at, shards_of in split:
        draws = jax.random.uniform(jax.random.fold_in(jax.random.fold_in(own_key, 6), axis_at), (shards_of,), jnp.float32, least / len(split), largest / len(split))
        gain = gain * jnp.repeat(jnp.exp(draws), shape[axis_at] // shards_of).reshape((-1,) + (1,) * (len(shape) - 1 - axis_at))
    return gain


def routed_block(stream_key, own, number, rows, count, top, limit, lean):
    order = jax.random.permutation(stream_key, count)
    heavy_load, usual = shares(count, rows * top, limit, lean, True), shares(count, rows * top, limit, lean, False)
    places = jnp.arange(count)

    def named(tallies, rotation):
        used = int((tallies > 0).sum())
        fixed = max(1, used // 4)
        shifted = fixed + (places - fixed + rotation * (used - fixed)) % max(1, count - fixed)
        return jnp.zeros((count,), jnp.int32).at[order[jnp.where(places < fixed, places, shifted)]].set(jnp.asarray(tallies, jnp.int32))

    tallies = jnp.where(number % 4 == 0, named(heavy_load, number // 4), named(usual, number - number // 4 - 1))
    mixed = jax.random.permutation(jax.random.fold_in(own, 3), count)
    source_of, taker = mixed[0:count // 2 * 2:2], mixed[1:count // 2 * 2:2]
    slack = jnp.minimum(tallies[source_of] - 1, limit - tallies[taker]) // 2
    slack = jnp.where((source_of == order[0]) | (taker == order[0]) | (tallies[taker] == 0), 0, jnp.maximum(slack, 0))
    shifted = jax.random.randint(jax.random.fold_in(own, 4), (count // 2,), 0, 1 << 20) % (slack + 1)
    tallies = tallies.at[source_of].add(-shifted).at[taker].add(shifted)
    labels = jnp.searchsorted(jnp.cumsum(tallies), jnp.arange(rows * top), side="right").astype(jnp.int32)
    table = labels.reshape(top, rows).T
    table = table[jax.random.permutation(jax.random.fold_in(own, 1), rows)]
    rotation = jax.random.randint(jax.random.fold_in(own, 2), (rows, 1), 0, top)
    return jnp.take_along_axis(table, (jnp.arange(top)[None, :] + rotation) % top, axis=1)


def shares(count, total, most, lean, full):
    weights = [(1 << 20) // math.isqrt(standing ** lean) + 1 for standing in range(1, count + 1)]
    largest = most if full else min(most, max(-(-total // count), total * weights[0] // sum(weights)))
    least = 1 if total - largest >= count - 1 else 0
    holding, spare = [largest] + [least] * (count - 1), total - largest - least * (count - 1)
    while spare > 0:
        candidates = [i for i in range(1, count) if holding[i] < largest] or [i for i in range(1, count) if holding[i] < most]
        whole, left = sum([weights[i] for i in candidates]), spare
        for i in candidates:
            addition = min(most - holding[i], max(1, left * weights[i] // whole), spare)
            holding[i] = holding[i] + addition
            spare = spare - addition
    return np.array(holding)


def centred(rng, dims, deviation, reach, cuts=(), held_as=jnp.bfloat16):
    array = jax.random.normal(rng, dims, jnp.float32) * deviation
    if len(cuts) > 0:
        array = block_scale(rng, dims, cuts, -0.22, 0.18) * array
    return jnp.clip(array, min=-reach, max=reach).astype(held_as)


def setup_inputs(seed: int = 0) -> dict:
    seeds = jax.random.split(jax.random.key(seed), 12)
    pooled_in = centred(seeds[0], (TOKENS, D_POOL), 1.0, 6.0, ((0, 64), (1, 4)))
    group_map = centred(seeds[1], (GROUPS, GROUP, GROUP), GROUP ** -0.5, 0.25, ((0, 4),))
    pool_scale = jnp.clip(1.0 + 0.18 * jax.random.normal(seeds[2], (D_POOL,), jnp.float32), 0.1, 1.9)
    out_weight = centred(seeds[3], (D_POOL, D), D_POOL ** -0.5, 0.125, ((0, 4),))
    residual = centred(seeds[4], (TOKENS, D), 1.0, 6.0, ((0, 256),))
    norm_gain = jnp.clip(1.0 + 0.18 * jax.random.normal(seeds[5], (D,), jnp.float32), 0.1, 1.9)
    gate_weight = centred(seeds[6], (EXPERTS, D, FF), D ** -0.5, 0.125, ((0, 64),))
    up_weight = centred(seeds[7], (EXPERTS, D, FF), D ** -0.5, 0.125, ((0, 64),))
    down_weight = centred(seeds[8], (EXPERTS, FF, D), FF ** -0.5, 0.25, ((0, 64),))
    route_expert_keys = jax.random.split(jax.random.fold_in(seeds[9], 1), TOKENS // ROWS_DEV)
    route_expert_turns = jax.random.permutation(jax.random.fold_in(seeds[9], 3), TOKENS // ROWS_DEV)
    route_expert = jax.vmap(lambda own, number: routed_block(jax.random.fold_in(seeds[9], 2), own, number, ROWS_DEV, EXPERTS, TOP, CAP, 2))(route_expert_keys, route_expert_turns).reshape((TOKENS, TOP))
    route_score = jnp.clip(jnp.exp(math.log(1.0) - 2.9957323 * jax.random.uniform(seeds[10], (TOKENS, TOP), jnp.float32) ** block_scale(seeds[10], (TOKENS, TOP), ((0, 256),), -0.2, 0.2)), 0.05, 1.0)
    return dict(pooled_in=pooled_in, group_map=group_map, pool_scale=pool_scale, out_weight=out_weight, residual=residual, norm_gain=norm_gain, gate_weight=gate_weight, up_weight=up_weight, down_weight=down_weight, route_expert=route_expert, route_score=route_score)


def reference(pooled_in, group_map, pool_scale, out_weight, residual, norm_gain, gate_weight, up_weight, down_weight, route_expert, route_score):
    columns = []
    for group_index in range(GROUPS):
        window = 2 ** (group_index + 1)
        channels = pooled_in[:, group_index * GROUP:(group_index + 1) * GROUP].astype(jnp.float32)
        padded = jnp.pad(channels, ((window - 1, 0), (0, 0)))
        running = jnp.zeros_like(channels)
        for offset in range(window):
            running = running + padded[window - 1 - offset:window - 1 - offset + TOKENS]
        counts = jnp.minimum(jnp.arange(TOKENS) + 1, window).astype(jnp.float32)
        contrast = (running / counts[:, None] - channels).astype(jnp.bfloat16)
        mixture = jnp.dot(contrast, group_map[group_index], preferred_element_type=jnp.float32)
        scales = pool_scale[group_index * GROUP:(group_index + 1) * GROUP]
        columns.append((mixture * scales[None, :]).astype(jnp.bfloat16))
    pooled = jnp.concatenate(columns, axis=1)
    projected = jnp.dot(pooled, out_weight, preferred_element_type=jnp.float32)
    middle = (residual.astype(jnp.float32) + projected).astype(jnp.bfloat16)
    middle_f = middle.astype(jnp.float32)
    factor = lax.rsqrt(lax.optimization_barrier(jnp.mean(middle_f * middle_f, axis=1, keepdims=True)) + 1e-06)
    normed = (middle_f * factor * norm_gain[None, :]).astype(jnp.bfloat16)
    share = route_score / lax.optimization_barrier(jnp.sum(route_score, axis=1, keepdims=True))
    blocks = TOKENS // ROWS_DEV
    assigned = route_expert.reshape(blocks, ROWS_DEV * TOP).astype(jnp.int32)
    onehot = (assigned[:, :, None] == jnp.arange(EXPERTS, dtype=jnp.int32)[None, None, :]).astype(jnp.int32)
    slot_rank = lax.optimization_barrier(jnp.sum(jnp.cumsum(onehot, axis=1) * onehot, axis=2)) - 1
    slot_index = (assigned * CAP + slot_rank).astype(jnp.int32)
    token_ids = (jnp.arange(blocks, dtype=jnp.int32)[:, None] * ROWS_DEV + jnp.arange(ROWS_DEV * TOP, dtype=jnp.int32)[None, :] // TOP).astype(jnp.int32)
    block_ids = jnp.broadcast_to(jnp.arange(blocks, dtype=jnp.int32)[:, None], slot_index.shape)
    slot_token = jnp.full((blocks, EXPERTS * CAP), TOKENS, jnp.int32).at[block_ids, slot_index].set(token_ids)
    slot_share = jnp.zeros((blocks, EXPERTS * CAP), jnp.float32).at[block_ids, slot_index].set(share.reshape(blocks, ROWS_DEV * TOP))
    token_by_expert = slot_token.reshape(blocks, EXPERTS, CAP).transpose(1, 0, 2).reshape(EXPERTS, blocks * CAP)
    share_by_expert = slot_share.reshape(blocks, EXPERTS, CAP).transpose(1, 0, 2).reshape(EXPERTS, blocks * CAP)
    padded_rows = jnp.concatenate([normed, jnp.zeros((1, D), jnp.bfloat16)], axis=0)

    def visit(totals, inputs):
        row_ids, row_share, gate_one, up_one, down_one = inputs
        rows_in = padded_rows[row_ids]
        gate_part = jnp.dot(rows_in, gate_one, preferred_element_type=jnp.float32)
        up_part = jnp.dot(rows_in, up_one, preferred_element_type=jnp.float32)
        hidden = (jax.nn.silu(gate_part) * up_part).astype(jnp.bfloat16)
        produced = jnp.dot(hidden, down_one, preferred_element_type=jnp.float32).astype(jnp.bfloat16)
        totals = totals.at[row_ids].add(produced.astype(jnp.float32) * row_share[:, None])
        return (totals, None)
    totals, _ = lax.scan(visit, jnp.zeros((TOKENS + 1, D), jnp.float32), (token_by_expert, share_by_expert, gate_weight, up_weight, down_weight))
    return (middle_f + totals[:TOKENS]).astype(jnp.bfloat16)
```

```python
import functools

import jax
import jax.numpy as jnp
from jax import lax
from jax.experimental import pallas as pl
from jax.experimental.pallas import tpu as pltpu
from jax.sharding import Mesh
from jax.sharding import PartitionSpec as P

AXES = ("z", "y", "c", "x")
SP = ("z", "y", "c")
MESH = pl.DeviceIdType.MESH
NZ, NY, NC, NX = 8, 4, 2, 4
NSP = NZ * NY * NC
HALO = 16
CAP = 12
BLK = 16
F32, BF16 = jnp.float32, jnp.bfloat16


def dot(a, b):
    return jnp.dot(a, b, preferred_element_type=F32)


def iota(shape, dim):
    return lax.broadcasted_iota(jnp.int32, shape, dim)


def kernel(
    pin_hbm, gm_ref, scale_ref, ow_hbm, res_hbm, gain_ref, wg_hbm, wu_hbm, wd_hbm, re_ref, sc_ref,
    out_ref,
    ext, ow, res, wg, wu, wd, pooled,
    s1, s2, r1, rl, rr, accp, accm, acc, middle, normed,
    mt, mtok, shr, onehot,
    send, recv, ret, back,
    lsem, halo_sem, rs_send, rs_recv, d_send, d_recv, b_send, b_recv,
):
    z, y, c, x = (lax.axis_index(a) for a in AXES)
    me = (z * NY + y) * NC + c
    rows = res_hbm.shape[0]
    width = res_hbm.shape[1]
    tok = pin_hbm.shape[0]
    half = width // 2
    q4 = width // 4

    def sp_peer(idx):
        return (idx // (NY * NC), (idx // NC) % NY, idx % NC, x)

    def x_peer(d):
        return (z, y, c, lax.rem(x + d, NX))

    barrier = pltpu.get_barrier_semaphore()

    def greet(k, carry):
        pl.semaphore_signal(
            barrier, inc=1, device_id=sp_peer(lax.rem(me + k, NSP)), device_id_type=MESH
        )
        return carry

    lax.fori_loop(1, NSP, greet, 0)
    for d in (1, NX - 1):
        pl.semaphore_signal(barrier, inc=1, device_id=x_peer(d), device_id_type=MESH)

    locals_ = [
        pltpu.make_async_copy(src, dst, lsem.at[i])
        for i, (src, dst) in enumerate(
            (
                (pin_hbm, ext.at[pl.ds(HALO, tok), :]),
                (ow_hbm, ow),
                (res_hbm, res),
                (wg_hbm, wg),
                (wu_hbm, wu),
                (wd_hbm, wd),
            )
        )
    ]
    for cp in locals_:
        cp.start()
    pl.semaphore_wait(barrier, NSP - 1 + 2)

    halo = pltpu.make_async_remote_copy(
        src_ref=pin_hbm.at[pl.ds(tok - HALO, HALO), :],
        dst_ref=ext.at[pl.ds(0, HALO), :],
        send_sem=halo_sem.at[0],
        recv_sem=halo_sem.at[1],
        device_id=sp_peer(lax.rem(me + 1, NSP)),
        device_id_type=MESH,
    )
    halo.start()

    lanes = 128
    el = iota((rows, lanes), 1)
    named0 = re_ref[:, 0:1] == el
    named1 = re_ref[:, 1:2] == el
    named = jnp.where(named0 | named1, 1.0, 0.0)
    before = jnp.where(iota((rows, rows), 1) < iota((rows, rows), 0), 1.0, 0.0).astype(BF16)
    rank = dot(before, named.astype(BF16))
    slot = jnp.where(named > 0.5, rank, -1.0)
    mtok[...] = slot.astype(BF16)
    mt[...] = jnp.transpose(slot)
    s0 = sc_ref[:, 0:1]
    s1v = sc_ref[:, 1:2]
    total = s0 + s1v
    shr[...] = (
        jnp.where(named0, s0 / total, 0.0) + jnp.where(named1, s1v / total, 0.0)
    ).astype(BF16)

    window = jnp.left_shift(jnp.int32(2), x)
    step = 128
    lag = iota((step, step + HALO), 0) + HALO - iota((step, step + HALO), 1)
    in_band = jnp.where((lag >= 0) & (lag < window), 1.0, 0.0)
    first_col = iota((step, step + HALO), 1) < HALO

    locals_[0].wait()
    halo.wait()

    def pool(b, carry):
        t0 = pl.multiple_of(b * step, step)
        start_of_all = (me == 0) & (b == 0)
        band = jnp.where(first_col & start_of_all, 0.0, in_band).astype(BF16)
        running = dot(band, ext[pl.ds(t0, step + HALO), :])
        pos = me * tok + t0 + iota((step, 1), 0)
        inverse = 1.0 / jnp.minimum(pos + 1, window).astype(F32)
        own = ext[pl.ds(t0 + HALO, step), :].astype(F32)
        contrast = (running * inverse - own).astype(BF16)
        mixture = dot(contrast, gm_ref[0])
        pooled[pl.ds(t0, step), :] = (mixture * scale_ref[...]).astype(BF16)
        return carry

    lax.fori_loop(0, tok // step, pool, 0)
    locals_[1].wait()

    def partial(d, col):
        base = pl.multiple_of(lax.rem(x + d, NX) * rows, rows)
        return dot(pooled[pl.ds(base, rows), :], ow[:, pl.ds(pl.multiple_of(col, 512), 512)])

    def rs_copy(i, src, dst, d):
        return pltpu.make_async_remote_copy(
            src_ref=src, dst_ref=dst, send_sem=rs_send.at[i], recv_sem=rs_recv.at[i],
            device_id=x_peer(d), device_id_type=MESH,
        )

    lo, hi = pl.ds(0, half), pl.ds(half, half)
    plus1 = rs_copy(0, s1.at[0], r1.at[0], 1)
    minus1 = rs_copy(1, s1.at[1], r1.at[1], NX - 1)
    plus2 = rs_copy(2, s2.at[0, 0], rl.at[1], 1)
    minus2 = rs_copy(3, s2.at[1, 0], rr.at[0], NX - 1)
    plus3 = rs_copy(4, s2.at[0, 1], rl.at[0], 1)
    minus3 = rs_copy(5, s2.at[1, 1], rr.at[1], NX - 1)

    def fill(j, carry):
        col = pl.multiple_of(j * 512, 512)
        s1[0, :, pl.ds(col, 512)] = partial(2, col).astype(BF16)
        s1[1, :, pl.ds(col, 512)] = partial(2, half + col).astype(BF16)
        return carry

    lax.fori_loop(0, half // 512, fill, 0)
    plus1.start()
    minus1.start()

    def fill2(j, carry):
        col = pl.multiple_of(j * 512, 512)
        s2[0, 0, :, pl.ds(col, 512)] = partial(1, half + col).astype(BF16)
        s2[1, 0, :, pl.ds(col, 512)] = partial(NX - 1, col).astype(BF16)
        return carry

    lax.fori_loop(0, half // 512, fill2, 0)
    plus2.start()
    minus2.start()

    def fill3(j, carry):
        col = pl.multiple_of(j * 512, 512)
        accp[:, pl.ds(col, 512)] = partial(1, col)
        accm[:, pl.ds(col, 512)] = partial(NX - 1, half + col)
        return carry

    lax.fori_loop(0, half // 512, fill3, 0)

    def fill4(j, carry):
        col = pl.multiple_of(j * 512, 512)
        acc[:, pl.ds(col, 512)] = partial(0, col)
        return carry

    lax.fori_loop(0, width // 512, fill4, 0)
    plus1.wait_recv()
    s2[0, 1] = (accp[...] + r1[0].astype(F32)).astype(BF16)
    plus3.start()
    minus1.wait_recv()
    s2[1, 1] = (accm[...] + r1[1].astype(F32)).astype(BF16)
    minus3.start()

    lane16 = lax.rem(iota((rows, lanes), 1), BLK)
    tail_at = 3 * (lane16 - CAP)

    def weights_of(g, carry):
        spread = jnp.where(iota((lanes, lanes), 0) == g * 8 + iota((lanes, lanes), 1) // BLK, 1.0, 0.0)
        spread = spread.astype(BF16)
        at = dot(mtok[...], spread)
        share = dot(shr[...], spread)
        for k in range(4):
            if k < 3:
                want = jnp.where(lane16 >= CAP, tail_at + k, -5)
            else:
                want = jnp.where(lane16 < CAP, lane16, -5)
            onehot[k, g] = jnp.where(at == want.astype(F32), share, 0.0).astype(BF16)
        return carry

    lax.fori_loop(0, NZ, weights_of, 0)

    locals_[2].wait()
    plus2.wait_recv()
    minus2.wait_recv()
    plus3.wait_recv()
    minus3.wait_recv()

    def norm(b, carry):
        at = pl.ds(pl.multiple_of(b * 32, 32), 32)
        halves = []
        for h in range(2):
            cols = pl.ds(h * half, half)
            projected = acc[at, cols] + rl[h, at, :].astype(F32) + rr[h, at, :].astype(F32)
            m = (res[at, cols].astype(F32) + projected).astype(BF16)
            middle[at, cols] = m
            halves.append(m.astype(F32))
        squares = sum(jnp.sum(m * m, axis=1, keepdims=True) for m in halves)
        factor = lax.rsqrt(squares / width + 1e-06)
        for h in range(2):
            cols = pl.ds(h * half, half)
            normed[at, cols] = (halves[h] * factor * gain_ref[:, cols]).astype(BF16)
        return carry

    lax.fori_loop(0, rows // 32, norm, 0)

    def dz_of(g):
        return 4 + ((g + 1) // 2) * (1 - 2 * lax.rem(g, 2))

    gl = 8 * BLK
    row16 = lax.rem(iota((gl, rows), 0), BLK)

    def block(idx):
        return pl.ds(pl.multiple_of(idx * BLK, BLK), BLK)

    def peer_index(zz, q):
        return (zz * NY + lax.rem(y + q // NC, NY)) * NC + lax.rem(c + q % NC, NC)

    def out_copy(dest):
        return pltpu.make_async_remote_copy(
            src_ref=send.at[block(dest), :], dst_ref=recv.at[block(me), :],
            send_sem=d_send.at[dest], recv_sem=d_recv.at[me],
            device_id=sp_peer(dest), device_id_type=MESH,
        )

    def out_wait(source):
        return pltpu.make_async_remote_copy(
            src_ref=send.at[block(source), :], dst_ref=recv.at[block(source), :],
            send_sem=d_send.at[source], recv_sem=d_recv.at[source],
            device_id=sp_peer(source), device_id_type=MESH,
        )

    def back_copy(dest):
        return pltpu.make_async_remote_copy(
            src_ref=ret.at[block(dest), :], dst_ref=back.at[block(me), :],
            send_sem=b_send.at[dest], recv_sem=b_recv.at[me],
            device_id=sp_peer(dest), device_id_type=MESH,
        )

    def back_wait(source):
        return pltpu.make_async_remote_copy(
            src_ref=ret.at[block(source), :], dst_ref=back.at[block(source), :],
            send_sem=b_send.at[source], recv_sem=b_recv.at[source],
            device_id=sp_peer(source), device_id_type=MESH,
        )

    def each_peer(g, zz, act):
        for q in range(8):
            idx = peer_index(zz, q)
            if q == 0:
                pl.when(g != NZ - 1)(functools.partial(act, idx))
            else:
                act(idx)

    def dispatch(g, carry):
        zz = lax.rem(z + dz_of(g), NZ)
        at8 = mt[pl.ds(pl.multiple_of(zz * 8, 8), 8), :]
        at = jnp.broadcast_to(at8[:, None, :], (8, BLK, rows)).reshape(gl, rows)
        main = jnp.where(at == jnp.where(row16 < CAP, row16, -5).astype(F32), 1.0, 0.0).astype(BF16)
        at_rows = pl.ds(pl.multiple_of(zz * gl, gl), gl)
        for k in range(3):
            want = jnp.where(row16 >= CAP, 3 * (row16 - CAP) + k, -5).astype(F32)
            tail = jnp.where(at == want, 1.0, 0.0).astype(BF16)
            cols = pl.ds(k * q4, q4)
            packed = dot(main, normed[:, cols]) + dot(tail, normed[:, pl.ds(3 * q4, q4)])
            send[at_rows, cols] = packed.astype(BF16)
        each_peer(g, zz, lambda idx: out_copy(idx).start())

        @pl.when(g == NZ - 1)
        def _():
            recv[block(me), :] = send[block(me), :]

        return carry

    lax.fori_loop(0, NZ, dispatch, 0)
    for i in (3, 4, 5):
        locals_[i].wait()

    ra, ca = iota((gl, gl), 0), iota((gl, gl), 1)
    same = ra // BLK == ca // BLK
    r16, c16 = lax.rem(ra, BLK), lax.rem(ca, BLK)
    keep = lax.rem(iota((gl, q4), 0), BLK) < CAP

    def ffn(g, carry):
        zz = lax.rem(z - dz_of(g) + 2 * NZ, NZ)
        each_peer(g, zz, lambda idx: out_wait(idx).wait_recv())
        at_rows = pl.ds(pl.multiple_of(zz * gl, gl), gl)
        tail = jnp.zeros((gl, q4), F32)
        for k in range(3):
            pick = jnp.where(same & (c16 >= CAP) & (r16 == 3 * (c16 - CAP) + k), 1.0, 0.0)
            tail = tail + dot(pick.astype(BF16), recv[at_rows, pl.ds(k * q4, q4)])
        tail = tail.astype(BF16)
        rows_in = recv[at_rows, :]
        gate = dot(rows_in, wg[pl.ds(0, 3 * q4), :]) + dot(tail, wg[pl.ds(3 * q4, q4), :])
        up = dot(rows_in, wu[pl.ds(0, 3 * q4), :]) + dot(tail, wu[pl.ds(3 * q4, q4), :])
        hidden = (gate / (1.0 + jnp.exp(-gate)) * up).astype(BF16)
        last = dot(hidden, wd[:, pl.ds(3 * q4, q4)]).astype(BF16)
        for k in range(3):
            put = jnp.where(same & (r16 >= CAP) & (c16 == 3 * (r16 - CAP) + k), 1.0, 0.0)
            cols = pl.ds(k * q4, q4)
            ret[at_rows, cols] = jnp.where(
                keep, dot(hidden, wd[:, cols]), dot(put.astype(BF16), last)
            ).astype(BF16)
        each_peer(g, zz, lambda idx: back_copy(idx).start())

        @pl.when(g == NZ - 1)
        def _():
            back[block(me), :] = ret[block(me), :]

        return carry

    lax.fori_loop(0, NZ, ffn, 0)

    def clear(b, carry):
        at = pl.ds(pl.multiple_of(b * 32, 32), 32)
        acc[at, :] = middle[at, :].astype(F32)
        return carry

    lax.fori_loop(0, rows // 32, clear, 0)

    def combine(g, carry):
        zz = lax.rem(z + dz_of(g), NZ)
        each_peer(g, zz, lambda idx: back_wait(idx).wait_recv())
        at_rows = pl.ds(pl.multiple_of(zz * gl, gl), gl)
        extra = acc[:, pl.ds(3 * q4, q4)]
        for k in range(3):
            cols = pl.ds(k * q4, q4)
            piece = back[at_rows, cols]
            acc[:, cols] += dot(onehot[3, zz], piece)
            extra = extra + dot(onehot[k, zz], piece)
        acc[:, pl.ds(3 * q4, q4)] = extra
        return carry

    lax.fori_loop(0, NZ, combine, 0)

    def finish(b, carry):
        at = pl.ds(pl.multiple_of(b * 32, 32), 32)
        out_ref[at, :] = acc[at, :].astype(BF16)
        return carry

    lax.fori_loop(0, rows // 32, finish, 0)
    for cp in (plus1, minus1, plus2, minus2, plus3, minus3):
        cp.wait_send()

    def drain(k, carry):
        idx = lax.rem(me + k, NSP)
        out_copy(idx).wait_send()
        back_copy(idx).wait_send()
        return carry

    lax.fori_loop(1, NSP, drain, 0)


def body(
    pooled_in, group_map, pool_scale, out_weight, residual, norm_gain,
    gate_weight, up_weight, down_weight, route_expert, route_score,
):
    tok, ch = pooled_in.shape
    rows, width = residual.shape
    ff = gate_weight.shape[2]
    half = width // 2
    packed = (NSP * BLK, 3 * width // 4)
    vmem = pl.BlockSpec(memory_space=pltpu.VMEM)
    hbm = pl.BlockSpec(memory_space=pl.ANY)
    dma = pltpu.SemaphoreType.DMA
    return pl.pallas_call(
        kernel,
        out_shape=jax.ShapeDtypeStruct((rows, width), BF16),
        in_specs=[hbm, vmem, vmem, hbm, hbm, vmem, hbm, hbm, hbm, vmem, vmem],
        out_specs=vmem,
        scratch_shapes=[
            pltpu.VMEM((HALO + tok, ch), BF16),
            pltpu.VMEM((ch, width), BF16),
            pltpu.VMEM((rows, width), BF16),
            pltpu.VMEM((width, ff), BF16),
            pltpu.VMEM((width, ff), BF16),
            pltpu.VMEM((ff, width), BF16),
            pltpu.VMEM((tok, ch), BF16),
            pltpu.VMEM((2, rows, half), BF16),
            pltpu.VMEM((2, 2, rows, half), BF16),
            pltpu.VMEM((2, rows, half), BF16),
            pltpu.VMEM((2, rows, half), BF16),
            pltpu.VMEM((2, rows, half), BF16),
            pltpu.VMEM((rows, half), F32),
            pltpu.VMEM((rows, half), F32),
            pltpu.VMEM((rows, width), F32),
            pltpu.VMEM((rows, width), BF16),
            pltpu.VMEM((rows, width), BF16),
            pltpu.VMEM((128, rows), F32),
            pltpu.VMEM((rows, 128), BF16),
            pltpu.VMEM((rows, 128), BF16),
            pltpu.VMEM((4, NZ, rows, 128), BF16),
            pltpu.VMEM(packed, BF16),
            pltpu.VMEM(packed, BF16),
            pltpu.VMEM(packed, BF16),
            pltpu.VMEM(packed, BF16),
            dma((6,)),
            dma((2,)),
            dma((6,)),
            dma((6,)),
            dma((NSP,)),
            dma((NSP,)),
            dma((NSP,)),
            dma((NSP,)),
        ],
        compiler_params=pltpu.CompilerParams(
            collective_id=0, has_side_effects=True, vmem_limit_bytes=60 * 2**20
        ),
    )(
        pooled_in, group_map, pool_scale.reshape(1, -1), out_weight, residual,
        norm_gain.reshape(1, -1), gate_weight.reshape(width, ff), up_weight.reshape(width, ff),
        down_weight.reshape(ff, width), route_expert, route_score,
    )


def solution(mesh):
    split = Mesh(mesh.devices.reshape(NZ, NY, NC, NX), AXES)
    sp_tp = AXES
    in_specs = (
        P(SP, "x"),
        P("x", None, None),
        P("x"),
        P("x", None),
        P(sp_tp, None),
        P(),
        P(SP, None, None),
        P(SP, None, None),
        P(SP, None, None),
        P(sp_tp, None),
        P(sp_tp, None),
    )
    return jax.shard_map(
        body, mesh=split, in_specs=in_specs, out_specs=P(sp_tp, None), check_vma=False
    )
```

```python
import functools

import jax
import jax.numpy as jnp
from jax import lax
from jax.experimental import pallas as pl
from jax.experimental.pallas import tpu as pltpu
from jax.sharding import Mesh
from jax.sharding import PartitionSpec as P

AXES = ("z", "y", "c", "x")
SP = ("z", "y", "c")
MESH = pl.DeviceIdType.MESH
NZ, NY, NC, NX = 8, 4, 2, 4
NSP = NZ * NY * NC
HALO = 16
CAP = 12
BLK = 16
F32, BF16 = jnp.float32, jnp.bfloat16


def dot(a, b):
    return jnp.dot(a, b, preferred_element_type=F32)


def iota(shape, dim):
    return lax.broadcasted_iota(jnp.int32, shape, dim)


def kernel(
    pin_hbm, gm_ref, scale_ref, ow_hbm, res_hbm, gain_ref, wg_hbm, wu_hbm, wd_hbm, re_ref, sc_ref,
    out_ref,
    ext, ow, res, wg, wu, wd, wg2, wu2, wd2, pooled,
    s1, s2, r1, rl, rr, accp, accm, acc, middle, normed,
    mt, mtok, shr, onehot,
    send, recv, ret, back,
    lsem, halo_sem, w_send, w_recv, rs_send, rs_recv, d_send, d_recv, b_send, b_recv,
):
    z, y, c, x = (lax.axis_index(a) for a in AXES)
    me = (z * NY + y) * NC + c
    rows = res_hbm.shape[0]
    width = res_hbm.shape[1]
    tok = pin_hbm.shape[0]
    half = width // 2
    q4 = width // 4

    def sp_peer(idx, xx=x):
        return (idx // (NY * NC), (idx // NC) % NY, idx % NC, xx)

    mirror = NX - 1 - x

    def x_peer(d):
        return (z, y, c, lax.rem(x + d, NX))

    barrier = pltpu.get_barrier_semaphore()

    def greet(k, carry):
        other = lax.rem(k, 2)
        pl.semaphore_signal(
            barrier,
            inc=1,
            device_id=sp_peer(lax.rem(me + k // 2, NSP), x + other * (mirror - x)),
            device_id_type=MESH,
        )
        return carry

    lax.fori_loop(1, 2 * NSP, greet, 0)
    pl.semaphore_signal(
        barrier, inc=1, device_id=(z, y, c, x + 1 - 2 * lax.rem(x, 2)), device_id_type=MESH
    )

    locals_ = [
        pltpu.make_async_copy(src, dst, lsem.at[i])
        for i, (src, dst) in enumerate(
            (
                (pin_hbm, ext.at[pl.ds(HALO, tok), :]),
                (ow_hbm, ow),
                (res_hbm, res),
                (wg_hbm, wg),
                (wu_hbm, wu),
                (wd_hbm, wd),
            )
        )
    ]
    for cp in locals_:
        cp.start()
    pl.semaphore_wait(barrier, 2 * NSP)

    gives = c == x // 2

    def weight_copy(i, side):
        src = (wg_hbm, wu_hbm, wd_hbm)[i]
        dst = (wg2, wu2, wd2)[i]
        return pltpu.make_async_remote_copy(
            src_ref=src, dst_ref=dst, send_sem=w_send.at[2 * i + side], recv_sem=w_recv.at[i],
            device_id=(lax.rem(z + (1, NZ - 1)[side], NZ), y, side, x), device_id_type=MESH,
        )

    @pl.when(gives)
    def _():
        for i in range(3):
            for side in range(2):
                weight_copy(i, side).start()

    halo = pltpu.make_async_remote_copy(
        src_ref=pin_hbm.at[pl.ds(tok - HALO, HALO), :],
        dst_ref=ext.at[pl.ds(0, HALO), :],
        send_sem=halo_sem.at[0],
        recv_sem=halo_sem.at[1],
        device_id=sp_peer(lax.rem(me + 1, NSP)),
        device_id_type=MESH,
    )
    halo.start()

    lanes = 128
    el = iota((rows, lanes), 1)
    named0 = re_ref[:, 0:1] == el
    named1 = re_ref[:, 1:2] == el
    named = jnp.where(named0 | named1, 1.0, 0.0)
    before = jnp.where(iota((rows, rows), 1) < iota((rows, rows), 0), 1.0, 0.0).astype(BF16)
    rank = dot(before, named.astype(BF16))
    slot = jnp.where(named > 0.5, rank, -1.0)
    mtok[...] = slot.astype(BF16)
    mt[...] = jnp.transpose(slot)
    s0 = sc_ref[:, 0:1]
    s1v = sc_ref[:, 1:2]
    total = s0 + s1v
    shr[...] = (
        jnp.where(named0, s0 / total, 0.0) + jnp.where(named1, s1v / total, 0.0)
    ).astype(BF16)

    window = jnp.left_shift(jnp.int32(2), x)
    step = 128
    lag = iota((step, step + HALO), 0) + HALO - iota((step, step + HALO), 1)
    in_band = jnp.where((lag >= 0) & (lag < window), 1.0, 0.0)
    first_col = iota((step, step + HALO), 1) < HALO

    locals_[0].wait()
    halo.wait()

    def pool(b, carry):
        t0 = pl.multiple_of(b * step, step)
        start_of_all = (me == 0) & (b == 0)
        band = jnp.where(first_col & start_of_all, 0.0, in_band).astype(BF16)
        running = dot(band, ext[pl.ds(t0, step + HALO), :])
        pos = me * tok + t0 + iota((step, 1), 0)
        inverse = 1.0 / jnp.minimum(pos + 1, window).astype(F32)
        own = ext[pl.ds(t0 + HALO, step), :].astype(F32)
        contrast = (running * inverse - own).astype(BF16)
        mixture = dot(contrast, gm_ref[0])
        pooled[pl.ds(t0, step), :] = (mixture * scale_ref[...]).astype(BF16)
        return carry

    lax.fori_loop(0, tok // step, pool, 0)
    locals_[1].wait()

    def partial(d, col):
        base = pl.multiple_of(lax.rem(x + d, NX) * rows, rows)
        return dot(pooled[pl.ds(base, rows), :], ow[:, pl.ds(pl.multiple_of(col, 512), 512)])

    def rs_copy(i, src, dst, d):
        return pltpu.make_async_remote_copy(
            src_ref=src, dst_ref=dst, send_sem=rs_send.at[i], recv_sem=rs_recv.at[i],
            device_id=x_peer(d), device_id_type=MESH,
        )

    lo, hi = pl.ds(0, half), pl.ds(half, half)
    plus1 = rs_copy(0, s1.at[0], r1.at[0], 1)
    minus1 = rs_copy(1, s1.at[1], r1.at[1], NX - 1)
    plus2 = rs_copy(2, s2.at[0, 0], rl.at[1], 1)
    minus2 = rs_copy(3, s2.at[1, 0], rr.at[0], NX - 1)
    plus3 = rs_copy(4, s2.at[0, 1], rl.at[0], 1)
    minus3 = rs_copy(5, s2.at[1, 1], rr.at[1], NX - 1)

    def fill(j, carry):
        col = pl.multiple_of(j * 512, 512)
        s1[0, :, pl.ds(col, 512)] = partial(2, col).astype(BF16)
        s1[1, :, pl.ds(col, 512)] = partial(2, half + col).astype(BF16)
        return carry

    lax.fori_loop(0, half // 512, fill, 0)
    plus1.start()
    minus1.start()

    def fill2(j, carry):
        col = pl.multiple_of(j * 512, 512)
        s2[0, 0, :, pl.ds(col, 512)] = partial(1, half + col).astype(BF16)
        s2[1, 0, :, pl.ds(col, 512)] = partial(NX - 1, col).astype(BF16)
        return carry

    lax.fori_loop(0, half // 512, fill2, 0)
    plus2.start()
    minus2.start()

    def fill3(j, carry):
        col = pl.multiple_of(j * 512, 512)
        accp[:, pl.ds(col, 512)] = partial(1, col)
        accm[:, pl.ds(col, 512)] = partial(NX - 1, half + col)
        return carry

    lax.fori_loop(0, half // 512, fill3, 0)

    def fill4(j, carry):
        col = pl.multiple_of(j * 512, 512)
        acc[:, pl.ds(col, 512)] = partial(0, col)
        return carry

    lax.fori_loop(0, width // 512, fill4, 0)
    plus1.wait_recv()
    s2[0, 1] = (accp[...] + r1[0].astype(F32)).astype(BF16)
    plus3.start()
    minus1.wait_recv()
    s2[1, 1] = (accm[...] + r1[1].astype(F32)).astype(BF16)
    minus3.start()

    lane16 = lax.rem(iota((rows, lanes), 1), BLK)
    tail_at = 3 * (lane16 - CAP)

    def weights_of(g, carry):
        spread = jnp.where(iota((lanes, lanes), 0) == g * 8 + iota((lanes, lanes), 1) // BLK, 1.0, 0.0)
        spread = spread.astype(BF16)
        at = dot(mtok[...], spread)
        share = dot(shr[...], spread)
        for k in range(4):
            if k < 3:
                want = jnp.where(lane16 >= CAP, tail_at + k, -5)
            else:
                want = jnp.where(lane16 < CAP, lane16, -5)
            onehot[k, g] = jnp.where(at == want.astype(F32), share, 0.0).astype(BF16)
        return carry

    lax.fori_loop(0, NZ, weights_of, 0)

    locals_[2].wait()
    plus2.wait_recv()
    minus2.wait_recv()
    plus3.wait_recv()
    minus3.wait_recv()

    def norm(b, carry):
        at = pl.ds(pl.multiple_of(b * 32, 32), 32)
        halves = []
        for h in range(2):
            cols = pl.ds(h * half, half)
            projected = acc[at, cols] + rl[h, at, :].astype(F32) + rr[h, at, :].astype(F32)
            m = (res[at, cols].astype(F32) + projected).astype(BF16)
            middle[at, cols] = m
            halves.append(m.astype(F32))
        squares = sum(jnp.sum(m * m, axis=1, keepdims=True) for m in halves)
        factor = lax.rsqrt(squares / width + 1e-06)
        for h in range(2):
            cols = pl.ds(h * half, half)
            normed[at, cols] = (halves[h] * factor * gain_ref[:, cols]).astype(BF16)
        return carry

    lax.fori_loop(0, rows // 32, norm, 0)

    def lag_of(g):
        return 4 + ((g + 1) // 2) * (1 - 2 * lax.rem(g, 2))

    gl = 8 * BLK
    row16 = lax.rem(iota((gl, rows), 0), BLK)
    sign = 1 - 2 * c

    def block(idx):
        return pl.ds(pl.multiple_of(idx * BLK, BLK), BLK)

    def place(lag, yy, cc):
        ze = lax.rem(z - lag + NZ, NZ)
        own = lag == 0
        plus = (lag < 4) | ((lag == 4) & (c == 0))
        shift = jnp.where(own, 0, jnp.where(plus, 1, NZ - 1))
        j = jnp.where(plus, lag - 1, 7 - lag)
        away = jnp.where(x // 2 == cc, 0, 1)
        core = jnp.where(own, cc, jnp.where(plus, 0, 1))
        xx = jnp.where(own | (away == 0), x, mirror)
        slot = jnp.where(
            own, y * 2 + c, jnp.where(j < 3, 8 + 16 * j + (y * 2 + c) * 2 + away, 56 + y * 2 + away)
        )
        dev = (lax.rem(ze + shift, NZ), yy, core, xx)
        return (ze * NY + yy) * NC + cc, dev, slot

    def is_me(dev):
        return (dev[0] == z) & (dev[1] == y) & (dev[2] == c) & (dev[3] == x)

    def origin(slot_group, yy, cc, away):
        if slot_group == "own":
            return (z, yy, cc, x), yy * 2 + cc, me
        j = slot_group
        zz = lax.rem(z + sign * j + NZ, NZ)
        xx = jnp.where(away == 0, x, mirror)
        slot = jnp.where(j < 3, 8 + 16 * j + (yy * 2 + cc) * 2 + away, 56 + yy * 2 + away)
        return (zz, yy, cc, xx), slot, imported

    imported = (lax.rem(z - sign + NZ, NZ) * NY + y) * NC + x // 2

    def members(group, act):
        if isinstance(group, str):
            todo = [(q // NC, q % NC, 0) for q in range(8)]
        elif isinstance(group, int):
            todo = [(q, c, away) for q in range(4) for away in range(2)]
        else:
            todo = [(q // NC, q % NC, away) for q in range(8) for away in range(2)]
        for q, cc, away in todo:
            core = cc if isinstance(group, int) else lax.rem(c + cc, NC)
            dev, slot, expert = origin(group, lax.rem(y + q, NY), core, away)
            pl.when(jnp.logical_not(is_me(dev)))(functools.partial(act, dev, slot, expert))

    def out_copy(expert, dev, slot):
        return pltpu.make_async_remote_copy(
            src_ref=send.at[block(expert), :], dst_ref=recv.at[block(slot), :],
            send_sem=d_send.at[expert], recv_sem=d_recv.at[slot],
            device_id=dev, device_id_type=MESH,
        )

    def back_copy(dev, slot, expert):
        return pltpu.make_async_remote_copy(
            src_ref=ret.at[block(slot), :], dst_ref=back.at[block(expert), :],
            send_sem=b_send.at[slot], recv_sem=b_recv.at[expert],
            device_id=dev, device_id_type=MESH,
        )

    def back_wait(expert, dev):
        return pltpu.make_async_remote_copy(
            src_ref=ret.at[block(expert), :], dst_ref=back.at[block(expert), :],
            send_sem=b_send.at[expert], recv_sem=b_recv.at[expert],
            device_id=dev, device_id_type=MESH,
        )

    def each_expert(lag, act):
        for q in range(8):
            expert, dev, slot = place(lag, lax.rem(y + q // NC, NY), lax.rem(c + q % NC, NC))
            pl.when(jnp.logical_not(is_me(dev)))(functools.partial(act, expert, dev, slot))

    def dispatch(g, carry):
        lag = lag_of(g)
        ze = lax.rem(z - lag + NZ, NZ)
        at8 = mt[pl.ds(pl.multiple_of(ze * 8, 8), 8), :]
        at = jnp.broadcast_to(at8[:, None, :], (8, BLK, rows)).reshape(gl, rows)
        main = jnp.where(at == jnp.where(row16 < CAP, row16, -5).astype(F32), 1.0, 0.0).astype(BF16)
        at_rows = pl.ds(pl.multiple_of(ze * gl, gl), gl)
        for k in range(3):
            want = jnp.where(row16 >= CAP, 3 * (row16 - CAP) + k, -5).astype(F32)
            tail = jnp.where(at == want, 1.0, 0.0).astype(BF16)
            cols = pl.ds(k * q4, q4)
            packed = dot(main, normed[:, cols]) + dot(tail, normed[:, pl.ds(3 * q4, q4)])
            send[at_rows, cols] = packed.astype(BF16)
        each_expert(lag, lambda expert, dev, slot: out_copy(expert, dev, slot).start())
        return carry

    lax.fori_loop(0, NZ, dispatch, 0)
    own_slot, far_slot = y * 2 + c, 8 + (y * 2 + c) * 2
    recv[block(own_slot), :] = send[block(me), :]
    recv[block(far_slot), :] = send[block(imported), :]
    for i in (3, 4, 5):
        locals_[i].wait()

    def ffn(group, first, count, gate_w, up_w, down_w):
        members(group, lambda dev, slot, expert: out_copy(slot, dev, slot).wait_recv())
        ra, ca = iota((count, count), 0), iota((count, count), 1)
        same = ra // BLK == ca // BLK
        r16, c16 = lax.rem(ra, BLK), lax.rem(ca, BLK)
        keep = lax.rem(iota((count, q4), 0), BLK) < CAP
        at_rows = pl.ds(pl.multiple_of(first * BLK, 128), count)
        tail = jnp.zeros((count, q4), F32)
        for k in range(3):
            pick = jnp.where(same & (c16 >= CAP) & (r16 == 3 * (c16 - CAP) + k), 1.0, 0.0)
            tail = tail + dot(pick.astype(BF16), recv[at_rows, pl.ds(k * q4, q4)])
        tail = tail.astype(BF16)
        rows_in = recv[at_rows, :]
        gate = dot(rows_in, gate_w[pl.ds(0, 3 * q4), :]) + dot(tail, gate_w[pl.ds(3 * q4, q4), :])
        up = dot(rows_in, up_w[pl.ds(0, 3 * q4), :]) + dot(tail, up_w[pl.ds(3 * q4, q4), :])
        hidden = (gate / (1.0 + jnp.exp(-gate)) * up).astype(BF16)
        last = dot(hidden, down_w[:, pl.ds(3 * q4, q4)]).astype(BF16)
        for k in range(3):
            put = jnp.where(same & (r16 >= CAP) & (c16 == 3 * (r16 - CAP) + k), 1.0, 0.0)
            cols = pl.ds(k * q4, q4)
            ret[at_rows, cols] = jnp.where(
                keep, dot(hidden, down_w[:, cols]), dot(put.astype(BF16), last)
            ).astype(BF16)
        members(group, lambda dev, slot, expert: back_copy(dev, slot, expert).start())

    ffn("own", 0, 8 * BLK, wg, wu, wd)
    back[block(me), :] = ret[block(own_slot), :]
    for i in range(3):
        weight_copy(i, 0).wait_recv()

    def far(i, carry):
        j = jnp.where(i == 0, 0, 3 - i)
        ffn(j, 8 + 16 * j, 16 * BLK, wg2, wu2, wd2)
        return carry

    lax.fori_loop(0, 1, far, 0)
    back[block(imported), :] = ret[block(far_slot), :]
    ffn(3, 56, 8 * BLK, wg2, wu2, wd2)
    lax.fori_loop(1, 3, far, 0)

    def clear(b, carry):
        at = pl.ds(pl.multiple_of(b * 32, 32), 32)
        acc[at, :] = middle[at, :].astype(F32)
        return carry

    lax.fori_loop(0, rows // 32, clear, 0)

    def combine(g, carry):
        lag = jnp.where(g < 2, g, jnp.where(g == 2, 7, jnp.where(g == 3, 4, jnp.where(
            g < 6, 2 * g - 5, 4 * g - 22))))
        zz = lax.rem(z - lag + NZ, NZ)
        each_expert(lag, lambda expert, dev, slot: back_wait(expert, dev).wait_recv())
        at_rows = pl.ds(pl.multiple_of(zz * gl, gl), gl)
        extra = acc[:, pl.ds(3 * q4, q4)]
        for k in range(3):
            cols = pl.ds(k * q4, q4)
            piece = back[at_rows, cols]
            acc[:, cols] += dot(onehot[3, zz], piece)
            extra = extra + dot(onehot[k, zz], piece)
        acc[:, pl.ds(3 * q4, q4)] = extra
        return carry

    lax.fori_loop(0, NZ, combine, 0)

    def finish(b, carry):
        at = pl.ds(pl.multiple_of(b * 32, 32), 32)
        out_ref[at, :] = acc[at, :].astype(BF16)
        return carry

    lax.fori_loop(0, rows // 32, finish, 0)
    for cp in (plus1, minus1, plus2, minus2, plus3, minus3):
        cp.wait_send()

    def drain(g, carry):
        each_expert(g, lambda expert, dev, slot: out_copy(expert, dev, slot).wait_send())
        return carry

    lax.fori_loop(0, NZ, drain, 0)
    members("own", lambda dev, slot, expert: back_copy(dev, slot, expert).wait_send())
    members(3, lambda dev, slot, expert: back_copy(dev, slot, expert).wait_send())

    def drain_far(j, carry):
        members(j, lambda dev, slot, expert: back_copy(dev, slot, expert).wait_send())
        return carry

    lax.fori_loop(0, 3, drain_far, 0)

    @pl.when(gives)
    def _():
        for i in range(3):
            for side in range(2):
                weight_copy(i, side).wait_send()


def body(
    pooled_in, group_map, pool_scale, out_weight, residual, norm_gain,
    gate_weight, up_weight, down_weight, route_expert, route_score,
):
    tok, ch = pooled_in.shape
    rows, width = residual.shape
    ff = gate_weight.shape[2]
    half = width // 2
    packed = (NSP * BLK, 3 * width // 4)
    vmem = pl.BlockSpec(memory_space=pltpu.VMEM)
    hbm = pl.BlockSpec(memory_space=pl.ANY)
    dma = pltpu.SemaphoreType.DMA
    return pl.pallas_call(
        kernel,
        out_shape=jax.ShapeDtypeStruct((rows, width), BF16),
        in_specs=[hbm, vmem, vmem, hbm, hbm, vmem, hbm, hbm, hbm, vmem, vmem],
        out_specs=vmem,
        scratch_shapes=[
            pltpu.VMEM((HALO + tok, ch), BF16),
            pltpu.VMEM((ch, width), BF16),
            pltpu.VMEM((rows, width), BF16),
            pltpu.VMEM((width, ff), BF16),
            pltpu.VMEM((width, ff), BF16),
            pltpu.VMEM((ff, width), BF16),
            pltpu.VMEM((width, ff), BF16),
            pltpu.VMEM((width, ff), BF16),
            pltpu.VMEM((ff, width), BF16),
            pltpu.VMEM((tok, ch), BF16),
            pltpu.VMEM((2, rows, half), BF16),
            pltpu.VMEM((2, 2, rows, half), BF16),
            pltpu.VMEM((2, rows, half), BF16),
            pltpu.VMEM((2, rows, half), BF16),
            pltpu.VMEM((2, rows, half), BF16),
            pltpu.VMEM((rows, half), F32),
            pltpu.VMEM((rows, half), F32),
            pltpu.VMEM((rows, width), F32),
            pltpu.VMEM((rows, width), BF16),
            pltpu.VMEM((rows, width), BF16),
            pltpu.VMEM((128, rows), F32),
            pltpu.VMEM((rows, 128), BF16),
            pltpu.VMEM((rows, 128), BF16),
            pltpu.VMEM((4, NZ, rows, 128), BF16),
            pltpu.VMEM(packed, BF16),
            pltpu.VMEM(packed, BF16),
            pltpu.VMEM(packed, BF16),
            pltpu.VMEM(packed, BF16),
            dma((6,)),
            dma((2,)),
            dma((6,)),
            dma((3,)),
            dma((6,)),
            dma((6,)),
            dma((NSP,)),
            dma((NSP,)),
            dma((NSP,)),
            dma((NSP,)),
        ],
        compiler_params=pltpu.CompilerParams(
            collective_id=0, has_side_effects=True, vmem_limit_bytes=60 * 2**20
        ),
    )(
        pooled_in, group_map, pool_scale.reshape(1, -1), out_weight, residual,
        norm_gain.reshape(1, -1), gate_weight.reshape(width, ff), up_weight.reshape(width, ff),
        down_weight.reshape(ff, width), route_expert, route_score,
    )


def solution(mesh):
    split = Mesh(mesh.devices.reshape(NZ, NY, NC, NX), AXES)
    sp_tp = AXES
    in_specs = (
        P(SP, "x"),
        P("x", None, None),
        P("x"),
        P("x", None),
        P(sp_tp, None),
        P(),
        P(SP, None, None),
        P(SP, None, None),
        P(SP, None, None),
        P(sp_tp, None),
        P(sp_tp, None),
    )
    return jax.shard_map(
        body, mesh=split, in_specs=in_specs, out_specs=P(sp_tp, None), check_vma=False
    )
```

```python
import functools

import jax
import jax.numpy as jnp
from jax import lax
from jax.experimental import pallas as pl
from jax.experimental.pallas import tpu as pltpu
from jax.sharding import Mesh
from jax.sharding import PartitionSpec as P

AXES = ("z", "y", "c", "x")
SP = ("z", "y", "c")
MESH = pl.DeviceIdType.MESH
NZ, NY, NC, NX = 8, 4, 2, 4
NSP = NZ * NY * NC
HALO = 16
CAP = 12
BLK = 16
F32, BF16 = jnp.float32, jnp.bfloat16


def dot(a, b):
    return jnp.dot(a, b, preferred_element_type=F32)


def iota(shape, dim):
    return lax.broadcasted_iota(jnp.int32, shape, dim)


def kernel(
    pin_hbm, gm_ref, scale_ref, ow_hbm, res_hbm, gain_ref, wg_hbm, wu_hbm, wd_hbm, re_ref, sc_ref,
    out_ref,
    ext, ow, res, wg, wu, wd, wg2, wu2, wd2, pooled,
    s1, s2, r1, rl, rr, accp, accm, acc, middle, normed,
    mt, mtok, shr, onehot,
    send, recv, ret, back,
    lsem, gate_sem, halo_sem, w_send, w_recv, rs_send, rs_recv, d_send, d_recv, b_send, b_recv,
):
    z, y, c, x = (lax.axis_index(a) for a in AXES)
    me = (z * NY + y) * NC + c
    rows = res_hbm.shape[0]
    width = res_hbm.shape[1]
    tok = pin_hbm.shape[0]
    half = width // 2
    q4 = width // 4

    def sp_peer(idx, xx=x):
        return (idx // (NY * NC), (idx // NC) % NY, idx % NC, xx)

    mirror = NX - 1 - x

    def x_peer(d):
        return (z, y, c, lax.rem(x + d, NX))

    barrier = pltpu.get_barrier_semaphore()

    lines = [(z, y, 1 - c, x), (z, y, c, mirror), (z, y, c, x + 1 - 2 * lax.rem(x, 2))]
    y_line = [(z, lax.rem(y + k, NY), c, x) for k in range(1, NY)]
    lines += y_line + [(lax.rem(z + k, NZ), y, c, x) for k in range(1, NZ)]
    lines.append(sp_peer(lax.rem(me + 2 * c - 1 + NSP, NSP)))
    lines += [(lax.rem(z + k, NZ), y, 1 - c, x) for k in (1, NZ - 1)]
    for dev in lines:
        pl.semaphore_signal(barrier, inc=1, device_id=dev, device_id_type=MESH)

    def stage(i, devs):
        for dev in devs:
            pl.semaphore_signal(gate_sem.at[i], inc=1, device_id=dev, device_id_type=MESH)
        pl.semaphore_wait(gate_sem.at[i], len(devs))

    locals_ = [
        pltpu.make_async_copy(src, dst, lsem.at[i])
        for i, (src, dst) in enumerate(
            (
                (pin_hbm, ext.at[pl.ds(HALO, tok), :]),
                (ow_hbm, ow),
                (res_hbm, res),
                (wg_hbm, wg),
                (wu_hbm, wu),
                (wd_hbm, wd),
            )
        )
    ]
    for cp in locals_:
        cp.start()
    pl.semaphore_wait(barrier, len(lines))

    halo = pltpu.make_async_remote_copy(
        src_ref=pin_hbm.at[pl.ds(tok - HALO, HALO), :],
        dst_ref=ext.at[pl.ds(0, HALO), :],
        send_sem=halo_sem.at[0],
        recv_sem=halo_sem.at[1],
        device_id=sp_peer(lax.rem(me + 1, NSP)),
        device_id_type=MESH,
    )
    halo.start()

    gives = c == x // 2

    def weight_copy(i, side):
        src = (wg_hbm, wu_hbm, wd_hbm)[i]
        dst = (wg2, wu2, wd2)[i]
        return pltpu.make_async_remote_copy(
            src_ref=src, dst_ref=dst, send_sem=w_send.at[2 * i + side], recv_sem=w_recv.at[i],
            device_id=(lax.rem(z + (1, NZ - 1)[side], NZ), y, side, x), device_id_type=MESH,
        )

    @pl.when(gives)
    def _():
        for i in range(3):
            for side in range(2):
                weight_copy(i, side).start()

    lanes = 128
    el = iota((rows, lanes), 1)
    mt[...] = jnp.zeros((lanes, rows), F32)
    mt[0:2, :] = re_ref[...].astype(F32)
    mt[2:4, :] = sc_ref[...]
    by_token = jnp.transpose(mt[...])
    el_f = el.astype(F32)
    named0 = by_token[:, 0:1] == el_f
    named1 = by_token[:, 1:2] == el_f
    named = jnp.where(named0 | named1, 1.0, 0.0)
    before = jnp.where(iota((rows, rows), 1) < iota((rows, rows), 0), 1.0, 0.0).astype(BF16)
    rank = dot(before, named.astype(BF16))
    slot = jnp.where(named > 0.5, rank, -1.0)
    mtok[...] = slot.astype(BF16)
    mt[...] = jnp.transpose(slot)
    s0 = by_token[:, 2:3]
    s1v = by_token[:, 3:4]
    total = s0 + s1v
    shr[...] = (
        jnp.where(named0, s0 / total, 0.0) + jnp.where(named1, s1v / total, 0.0)
    ).astype(BF16)

    window = jnp.left_shift(jnp.int32(2), x)
    step = 128
    lag = iota((step, step + HALO), 0) + HALO - iota((step, step + HALO), 1)
    in_band = jnp.where((lag >= 0) & (lag < window), 1.0, 0.0)
    first_col = iota((step, step + HALO), 1) < HALO

    stage(0, y_line)
    locals_[0].wait()
    halo.wait()

    def pool(b, carry):
        t0 = pl.multiple_of(b * step, step)
        start_of_all = (me == 0) & (b == 0)
        band = jnp.where(first_col & start_of_all, 0.0, in_band).astype(BF16)
        running = dot(band, ext[pl.ds(t0, step + HALO), :])
        pos = me * tok + t0 + iota((step, 1), 0)
        inverse = 1.0 / jnp.minimum(pos + 1, window).astype(F32)
        own = ext[pl.ds(t0 + HALO, step), :].astype(F32)
        contrast = (running * inverse - own).astype(BF16)
        mixture = dot(contrast, gm_ref[0])
        pooled[pl.ds(t0, step), :] = (mixture * scale_ref[...]).astype(BF16)
        return carry

    lax.fori_loop(0, tok // step, pool, 0)
    stage(1, lines[:1])
    locals_[1].wait()

    def partial(d, col):
        base = pl.multiple_of(lax.rem(x + d, NX) * rows, rows)
        return dot(pooled[pl.ds(base, rows), :], ow[:, pl.ds(pl.multiple_of(col, 512), 512)])

    def rs_copy(i, src, dst, d):
        return pltpu.make_async_remote_copy(
            src_ref=src, dst_ref=dst, send_sem=rs_send.at[i], recv_sem=rs_recv.at[i],
            device_id=x_peer(d), device_id_type=MESH,
        )

    lo, hi = pl.ds(0, half), pl.ds(half, half)
    plus1 = rs_copy(0, s1.at[0], r1.at[0], 1)
    minus1 = rs_copy(1, s1.at[1], r1.at[1], NX - 1)
    plus2 = rs_copy(2, s2.at[0, 0], rl.at[1], 1)
    minus2 = rs_copy(3, s2.at[1, 0], rr.at[0], NX - 1)
    plus3 = rs_copy(4, s2.at[0, 1], rl.at[0], 1)
    minus3 = rs_copy(5, s2.at[1, 1], rr.at[1], NX - 1)

    def fill(j, carry):
        col = pl.multiple_of(j * 512, 512)
        s1[0, :, pl.ds(col, 512)] = partial(2, col).astype(BF16)
        s1[1, :, pl.ds(col, 512)] = partial(2, half + col).astype(BF16)
        return carry

    lax.fori_loop(0, half // 512, fill, 0)
    plus1.start()
    minus1.start()
    stage(2, lines[1:2])

    def fill2(j, carry):
        col = pl.multiple_of(j * 512, 512)
        s2[0, 0, :, pl.ds(col, 512)] = partial(1, half + col).astype(BF16)
        s2[1, 0, :, pl.ds(col, 512)] = partial(NX - 1, col).astype(BF16)
        return carry

    lax.fori_loop(0, half // 512, fill2, 0)
    plus2.start()
    minus2.start()

    def fill3(j, carry):
        col = pl.multiple_of(j * 512, 512)
        accp[:, pl.ds(col, 512)] = partial(1, col)
        accm[:, pl.ds(col, 512)] = partial(NX - 1, half + col)
        return carry

    lax.fori_loop(0, half // 512, fill3, 0)

    def fill4(j, carry):
        col = pl.multiple_of(j * 512, 512)
        acc[:, pl.ds(col, 512)] = partial(0, col)
        return carry

    lax.fori_loop(0, width // 512, fill4, 0)
    plus1.wait_recv()
    s2[0, 1] = (accp[...] + r1[0].astype(F32)).astype(BF16)
    plus3.start()
    minus1.wait_recv()
    s2[1, 1] = (accm[...] + r1[1].astype(F32)).astype(BF16)
    minus3.start()

    lane16 = lax.rem(iota((rows, lanes), 1), BLK)
    tail_at = 3 * (lane16 - CAP)

    def weights_of(g, carry):
        spread = jnp.where(iota((lanes, lanes), 0) == g * 8 + iota((lanes, lanes), 1) // BLK, 1.0, 0.0)
        spread = spread.astype(BF16)
        at = dot(mtok[...], spread)
        share = dot(shr[...], spread)
        for k in range(4):
            if k < 3:
                want = jnp.where(lane16 >= CAP, tail_at + k, -5)
            else:
                want = jnp.where(lane16 < CAP, lane16, -5)
            onehot[k, g] = jnp.where(at == want.astype(F32), share, 0.0).astype(BF16)
        return carry

    lax.fori_loop(0, NZ, weights_of, 0)

    locals_[2].wait()
    plus2.wait_recv()
    minus2.wait_recv()
    plus3.wait_recv()
    minus3.wait_recv()

    def norm(b, carry):
        at = pl.ds(pl.multiple_of(b * 32, 32), 32)
        halves = []
        for h in range(2):
            cols = pl.ds(h * half, half)
            projected = acc[at, cols] + rl[h, at, :].astype(F32) + rr[h, at, :].astype(F32)
            m = (res[at, cols].astype(F32) + projected).astype(BF16)
            middle[at, cols] = m
            halves.append(m.astype(F32))
        squares = sum(jnp.sum(m * m, axis=1, keepdims=True) for m in halves)
        factor = lax.rsqrt(squares / width + 1e-06)
        for h in range(2):
            cols = pl.ds(h * half, half)
            normed[at, cols] = (halves[h] * factor * gain_ref[:, cols]).astype(BF16)
        return carry

    lax.fori_loop(0, rows // 32, norm, 0)

    def lag_of(g):
        return 4 + ((g + 1) // 2) * (1 - 2 * lax.rem(g, 2))

    gl = 8 * BLK
    row16 = lax.rem(iota((gl, rows), 0), BLK)
    sign = 1 - 2 * c

    def block(idx):
        return pl.ds(pl.multiple_of(idx * BLK, BLK), BLK)

    def place(lag, yy, cc):
        ze = lax.rem(z - lag + NZ, NZ)
        own = lag == 0
        plus = (lag < 4) | ((lag == 4) & (c == 0))
        shift = jnp.where(own, 0, jnp.where(plus, 1, NZ - 1))
        j = jnp.where(plus, lag - 1, 7 - lag)
        away = jnp.where(x // 2 == cc, 0, 1)
        core = jnp.where(own, cc, jnp.where(plus, 0, 1))
        xx = jnp.where(own | (away == 0), x, mirror)
        slot = jnp.where(
            own, y * 2 + c, jnp.where(j < 3, 8 + 16 * j + (y * 2 + c) * 2 + away, 56 + y * 2 + away)
        )
        dev = (lax.rem(ze + shift, NZ), yy, core, xx)
        return (ze * NY + yy) * NC + cc, dev, slot

    def is_me(dev):
        return (dev[0] == z) & (dev[1] == y) & (dev[2] == c) & (dev[3] == x)

    def origin(slot_group, yy, cc, away):
        if slot_group == "own":
            return (z, yy, cc, x), yy * 2 + cc, me
        j = slot_group
        zz = lax.rem(z + sign * j + NZ, NZ)
        xx = jnp.where(away == 0, x, mirror)
        slot = jnp.where(j < 3, 8 + 16 * j + (yy * 2 + cc) * 2 + away, 56 + yy * 2 + away)
        return (zz, yy, cc, xx), slot, imported

    imported = (lax.rem(z - sign + NZ, NZ) * NY + y) * NC + x // 2

    def members(group, act):
        if isinstance(group, str):
            todo = [(q // NC, q % NC, 0) for q in range(8)]
        elif isinstance(group, int):
            todo = [(q, c, away) for q in range(4) for away in range(2)]
        else:
            todo = [(q // NC, q % NC, away) for q in range(8) for away in range(2)]
        for q, cc, away in todo:
            core = cc if isinstance(group, int) else lax.rem(c + cc, NC)
            dev, slot, expert = origin(group, lax.rem(y + q, NY), core, away)
            pl.when(jnp.logical_not(is_me(dev)))(functools.partial(act, dev, slot, expert))

    def out_copy(expert, dev, slot):
        return pltpu.make_async_remote_copy(
            src_ref=send.at[block(expert), :], dst_ref=recv.at[block(slot), :],
            send_sem=d_send.at[expert], recv_sem=d_recv.at[slot],
            device_id=dev, device_id_type=MESH,
        )

    def back_copy(dev, slot, expert):
        return pltpu.make_async_remote_copy(
            src_ref=ret.at[block(slot), :], dst_ref=back.at[block(expert), :],
            send_sem=b_send.at[slot], recv_sem=b_recv.at[expert],
            device_id=dev, device_id_type=MESH,
        )

    def back_wait(expert, dev):
        return pltpu.make_async_remote_copy(
            src_ref=ret.at[block(expert), :], dst_ref=back.at[block(expert), :],
            send_sem=b_send.at[expert], recv_sem=b_recv.at[expert],
            device_id=dev, device_id_type=MESH,
        )

    def each_expert(lag, act):
        for q in range(8):
            expert, dev, slot = place(lag, lax.rem(y + q // NC, NY), lax.rem(c + q % NC, NC))
            pl.when(jnp.logical_not(is_me(dev)))(functools.partial(act, expert, dev, slot))

    def dispatch(g, carry):
        lag = lag_of(g)
        ze = lax.rem(z - lag + NZ, NZ)
        at8 = mt[pl.ds(pl.multiple_of(ze * 8, 8), 8), :]
        at = jnp.broadcast_to(at8[:, None, :], (8, BLK, rows)).reshape(gl, rows)
        main = jnp.where(at == jnp.where(row16 < CAP, row16, -5).astype(F32), 1.0, 0.0).astype(BF16)
        at_rows = pl.ds(pl.multiple_of(ze * gl, gl), gl)
        for k in range(3):
            want = jnp.where(row16 >= CAP, 3 * (row16 - CAP) + k, -5).astype(F32)
            tail = jnp.where(at == want, 1.0, 0.0).astype(BF16)
            cols = pl.ds(k * q4, q4)
            packed = dot(main, normed[:, cols]) + dot(tail, normed[:, pl.ds(3 * q4, q4)])
            send[at_rows, cols] = packed.astype(BF16)
        each_expert(lag, lambda expert, dev, slot: out_copy(expert, dev, slot).start())
        return carry

    lax.fori_loop(0, NZ, dispatch, 0)
    own_slot, far_slot = y * 2 + c, 8 + (y * 2 + c) * 2
    recv[block(own_slot), :] = send[block(me), :]
    recv[block(far_slot), :] = send[block(imported), :]
    for i in (3, 4, 5):
        locals_[i].wait()

    def ffn(group, first, count, gate_w, up_w, down_w):
        members(group, lambda dev, slot, expert: out_copy(slot, dev, slot).wait_recv())
        ra, ca = iota((count, count), 0), iota((count, count), 1)
        same = ra // BLK == ca // BLK
        r16, c16 = lax.rem(ra, BLK), lax.rem(ca, BLK)
        keep = lax.rem(iota((count, q4), 0), BLK) < CAP
        at_rows = pl.ds(pl.multiple_of(first * BLK, 128), count)
        tail = jnp.zeros((count, q4), F32)
        for k in range(3):
            pick = jnp.where(same & (c16 >= CAP) & (r16 == 3 * (c16 - CAP) + k), 1.0, 0.0)
            tail = tail + dot(pick.astype(BF16), recv[at_rows, pl.ds(k * q4, q4)])
        tail = tail.astype(BF16)
        rows_in = recv[at_rows, :]
        gate = dot(rows_in, gate_w[pl.ds(0, 3 * q4), :]) + dot(tail, gate_w[pl.ds(3 * q4, q4), :])
        up = dot(rows_in, up_w[pl.ds(0, 3 * q4), :]) + dot(tail, up_w[pl.ds(3 * q4, q4), :])
        hidden = (gate / (1.0 + jnp.exp(-gate)) * up).astype(BF16)
        last = dot(hidden, down_w[:, pl.ds(3 * q4, q4)]).astype(BF16)
        for k in range(3):
            put = jnp.where(same & (r16 >= CAP) & (c16 == 3 * (r16 - CAP) + k), 1.0, 0.0)
            cols = pl.ds(k * q4, q4)
            ret[at_rows, cols] = jnp.where(
                keep, dot(hidden, down_w[:, cols]), dot(put.astype(BF16), last)
            ).astype(BF16)
        members(group, lambda dev, slot, expert: back_copy(dev, slot, expert).start())

    ffn("own", 0, 8 * BLK, wg, wu, wd)
    back[block(me), :] = ret[block(own_slot), :]
    for i in range(3):
        weight_copy(i, 0).wait_recv()

    def far(i, carry):
        j = jnp.where(i == 0, 0, 3 - i)
        ffn(j, 8 + 16 * j, 16 * BLK, wg2, wu2, wd2)
        return carry

    lax.fori_loop(0, 1, far, 0)
    back[block(imported), :] = ret[block(far_slot), :]
    ffn(3, 56, 8 * BLK, wg2, wu2, wd2)
    lax.fori_loop(1, 3, far, 0)

    def clear(b, carry):
        at = pl.ds(pl.multiple_of(b * 32, 32), 32)
        acc[at, :] = middle[at, :].astype(F32)
        return carry

    lax.fori_loop(0, rows // 32, clear, 0)

    def combine(g, carry):
        lag = jnp.where(g < 2, g, jnp.where(g == 2, 7, jnp.where(g == 3, 4, jnp.where(
            g < 6, 2 * g - 5, 4 * g - 22))))
        zz = lax.rem(z - lag + NZ, NZ)
        each_expert(lag, lambda expert, dev, slot: back_wait(expert, dev).wait_recv())
        at_rows = pl.ds(pl.multiple_of(zz * gl, gl), gl)
        extra = acc[:, pl.ds(3 * q4, q4)]
        for k in range(3):
            cols = pl.ds(k * q4, q4)
            piece = back[at_rows, cols]
            acc[:, cols] += dot(onehot[3, zz], piece)
            extra = extra + dot(onehot[k, zz], piece)
        acc[:, pl.ds(3 * q4, q4)] = extra
        return carry

    lax.fori_loop(0, NZ, combine, 0)

    def finish(b, carry):
        at = pl.ds(pl.multiple_of(b * 32, 32), 32)
        out_ref[at, :] = acc[at, :].astype(BF16)
        return carry

    lax.fori_loop(0, rows // 32, finish, 0)
    for cp in (plus1, minus1, plus2, minus2, plus3, minus3):
        cp.wait_send()

    def drain(g, carry):
        each_expert(g, lambda expert, dev, slot: out_copy(expert, dev, slot).wait_send())
        return carry

    lax.fori_loop(0, NZ, drain, 0)
    members("own", lambda dev, slot, expert: back_copy(dev, slot, expert).wait_send())
    members(3, lambda dev, slot, expert: back_copy(dev, slot, expert).wait_send())

    def drain_far(j, carry):
        members(j, lambda dev, slot, expert: back_copy(dev, slot, expert).wait_send())
        return carry

    lax.fori_loop(0, 3, drain_far, 0)

    @pl.when(gives)
    def _():
        for i in range(3):
            for side in range(2):
                weight_copy(i, side).wait_send()


def body(
    pooled_in, group_map, pool_scale, out_weight, residual, norm_gain,
    gate_weight, up_weight, down_weight, route_expert, route_score,
):
    tok, ch = pooled_in.shape
    rows, width = residual.shape
    ff = gate_weight.shape[2]
    half = width // 2
    packed = (NSP * BLK, 3 * width // 4)
    vmem = pl.BlockSpec(memory_space=pltpu.VMEM)
    hbm = pl.BlockSpec(memory_space=pl.ANY)
    dma = pltpu.SemaphoreType.DMA
    return pl.pallas_call(
        kernel,
        out_shape=jax.ShapeDtypeStruct((rows, width), BF16),
        in_specs=[hbm, vmem, vmem, hbm, hbm, vmem, hbm, hbm, hbm, vmem, vmem],
        out_specs=vmem,
        scratch_shapes=[
            pltpu.VMEM((HALO + tok, ch), BF16),
            pltpu.VMEM((ch, width), BF16),
            pltpu.VMEM((rows, width), BF16),
            pltpu.VMEM((width, ff), BF16),
            pltpu.VMEM((width, ff), BF16),
            pltpu.VMEM((ff, width), BF16),
            pltpu.VMEM((width, ff), BF16),
            pltpu.VMEM((width, ff), BF16),
            pltpu.VMEM((ff, width), BF16),
            pltpu.VMEM((tok, ch), BF16),
            pltpu.VMEM((2, rows, half), BF16),
            pltpu.VMEM((2, 2, rows, half), BF16),
            pltpu.VMEM((2, rows, half), BF16),
            pltpu.VMEM((2, rows, half), BF16),
            pltpu.VMEM((2, rows, half), BF16),
            pltpu.VMEM((rows, half), F32),
            pltpu.VMEM((rows, half), F32),
            pltpu.VMEM((rows, width), F32),
            pltpu.VMEM((rows, width), BF16),
            pltpu.VMEM((rows, width), BF16),
            pltpu.VMEM((128, rows), F32),
            pltpu.VMEM((rows, 128), BF16),
            pltpu.VMEM((rows, 128), BF16),
            pltpu.VMEM((4, NZ, rows, 128), BF16),
            pltpu.VMEM(packed, BF16),
            pltpu.VMEM(packed, BF16),
            pltpu.VMEM(packed, BF16),
            pltpu.VMEM(packed, BF16),
            dma((6,)),
            pltpu.SemaphoreType.REGULAR((3,)),
            dma((2,)),
            dma((6,)),
            dma((3,)),
            dma((6,)),
            dma((6,)),
            dma((NSP,)),
            dma((NSP,)),
            dma((NSP,)),
            dma((NSP,)),
        ],
        compiler_params=pltpu.CompilerParams(
            collective_id=0, has_side_effects=True, vmem_limit_bytes=60 * 2**20
        ),
    )(
        pooled_in, group_map, pool_scale.reshape(1, -1), out_weight, residual,
        norm_gain.reshape(1, -1), gate_weight.reshape(width, ff), up_weight.reshape(width, ff),
        down_weight.reshape(ff, width), route_expert.T, route_score.T,
    )


def solution(mesh):
    split = Mesh(mesh.devices.reshape(NZ, NY, NC, NX), AXES)
    sp_tp = AXES
    in_specs = (
        P(SP, "x"),
        P("x", None, None),
        P("x"),
        P("x", None),
        P(sp_tp, None),
        P(),
        P(SP, None, None),
        P(SP, None, None),
        P(SP, None, None),
        P(sp_tp, None),
        P(sp_tp, None),
    )
    return jax.shard_map(
        body, mesh=split, in_specs=in_specs, out_specs=P(sp_tp, None), check_vma=False
    )
```

```python
import functools

import jax
import jax.numpy as jnp
from jax import lax
from jax.experimental import pallas as pl
from jax.experimental.pallas import tpu as pltpu
from jax.sharding import Mesh
from jax.sharding import PartitionSpec as P

AXES = ("z", "y", "c", "x")
SP = ("z", "y", "c")
MESH = pl.DeviceIdType.MESH
NZ, NY, NC, NX = 8, 4, 2, 4
NSP = NZ * NY * NC
HALO = 16
CAP = 12
BLK = 16
F32, BF16 = jnp.float32, jnp.bfloat16


def dot(a, b):
    return jnp.dot(a, b, preferred_element_type=F32)


def iota(shape, dim):
    return lax.broadcasted_iota(jnp.int32, shape, dim)


def kernel(
    pin_hbm, gm_ref, scale_ref, ow_hbm, res_hbm, gain_ref, wg_hbm, wu_hbm, wd_hbm, re_ref, sc_ref,
    out_ref,
    ext, ow, res, wg, wu, wd, wg2, wu2, wd2, pooled,
    s1, s2, r1, rl, rr, accp, accm, acc, middle, normed,
    mt, mtok, shr, onehot,
    send, recv, ret, back,
    lsem, gate_sem, halo_sem, swap_sem, w_send, w_recv, rs_send, rs_recv, d_send, d_recv, b_send, b_recv,
):
    z, y, c, x = (lax.axis_index(a) for a in AXES)
    me = (z * NY + y) * NC + c
    rows = res_hbm.shape[0]
    width = res_hbm.shape[1]
    tok = pin_hbm.shape[0]
    half = width // 2
    q4 = width // 4

    def sp_peer(idx, xx=x):
        return (idx // (NY * NC), (idx // NC) % NY, idx % NC, xx)

    mirror = NX - 1 - x

    def x_peer(d):
        return (z, y, c, lax.rem(x + d, NX))

    barrier = pltpu.get_barrier_semaphore()

    lines = [(z, y, 1 - c, x), (z, y, c, mirror), (z, y, c, x + 1 - 2 * lax.rem(x, 2))]
    y_line = [(z, lax.rem(y + k, NY), c, x) for k in range(1, NY)]
    lines += y_line + [(lax.rem(z + k, NZ), y, c, x) for k in range(1, NZ)]
    lines.append(sp_peer(lax.rem(me + 2 * c - 1 + NSP, NSP)))
    lines += [(lax.rem(z + k, NZ), y, 1 - c, x) for k in (1, NZ - 1)]
    for dev in lines:
        pl.semaphore_signal(barrier, inc=1, device_id=dev, device_id_type=MESH)

    def stage(i, devs):
        for dev in devs:
            pl.semaphore_signal(gate_sem.at[i], inc=1, device_id=dev, device_id_type=MESH)
        pl.semaphore_wait(gate_sem.at[i], len(devs))

    locals_ = [
        pltpu.make_async_copy(src, dst, lsem.at[i])
        for i, (src, dst) in enumerate(
            (
                (pin_hbm, ext.at[pl.ds(HALO, tok), :]),
                (ow_hbm, ow),
                (res_hbm, res),
                (wg_hbm, wg),
                (wu_hbm, wu),
                (wd_hbm, wd),
            )
        )
    ]
    for cp in locals_:
        cp.start()
    pl.semaphore_wait(barrier, len(lines))

    halo = pltpu.make_async_remote_copy(
        src_ref=pin_hbm.at[pl.ds(tok - HALO, HALO), :],
        dst_ref=ext.at[pl.ds(0, HALO), :],
        send_sem=halo_sem.at[0],
        recv_sem=halo_sem.at[1],
        device_id=sp_peer(lax.rem(me + 1, NSP)),
        device_id_type=MESH,
    )
    halo.start()

    gives = c == x // 2

    mid = wd_hbm.shape[0] // 2
    pair = x + 1 - 2 * lax.rem(x, 2)

    def my_half(ref):
        return ref.at[pl.ds(pl.multiple_of(lax.rem(x, 2) * mid, mid), mid), :]

    def weight_copy(i, side):
        src = (my_half(wd_hbm), wg_hbm, wu_hbm)[i]
        dst = (my_half(wd2), wg2, wu2)[i]
        return pltpu.make_async_remote_copy(
            src_ref=src, dst_ref=dst, send_sem=w_send.at[2 * i + side], recv_sem=w_recv.at[i],
            device_id=(lax.rem(z + (1, NZ - 1)[side], NZ), y, side, x), device_id_type=MESH,
        )

    swap = pltpu.make_async_remote_copy(
        src_ref=my_half(wd2), dst_ref=my_half(wd2), send_sem=swap_sem.at[0], recv_sem=swap_sem.at[1],
        device_id=(z, y, c, pair), device_id_type=MESH,
    )

    @pl.when(gives)
    def _():
        for i in range(3):
            for side in range(2):
                weight_copy(i, side).start()

    lanes = 128
    el = iota((rows, lanes), 1)
    mt[...] = jnp.zeros((lanes, rows), F32)
    mt[0:2, :] = re_ref[...].astype(F32)
    mt[2:4, :] = sc_ref[...]
    by_token = jnp.transpose(mt[...])
    el_f = el.astype(F32)
    named0 = by_token[:, 0:1] == el_f
    named1 = by_token[:, 1:2] == el_f
    named = jnp.where(named0 | named1, 1.0, 0.0)
    before = jnp.where(iota((rows, rows), 1) < iota((rows, rows), 0), 1.0, 0.0).astype(BF16)
    rank = dot(before, named.astype(BF16))
    slot = jnp.where(named > 0.5, rank, -1.0)
    mtok[...] = slot.astype(BF16)
    mt[...] = jnp.transpose(slot)
    s0 = by_token[:, 2:3]
    s1v = by_token[:, 3:4]
    total = s0 + s1v
    shr[...] = (
        jnp.where(named0, s0 / total, 0.0) + jnp.where(named1, s1v / total, 0.0)
    ).astype(BF16)

    window = jnp.left_shift(jnp.int32(2), x)
    step = 128
    lag = iota((step, step + HALO), 0) + HALO - iota((step, step + HALO), 1)
    in_band = jnp.where((lag >= 0) & (lag < window), 1.0, 0.0)
    first_col = iota((step, step + HALO), 1) < HALO

    stage(0, y_line)
    locals_[0].wait()
    halo.wait_recv()

    per = rows // step

    def pool(i, carry):
        part = i // per
        d = jnp.where(part == 0, 2, jnp.where(part == 3, 0, 2 * part - 1))
        b = lax.rem(x + d, NX) * per + lax.rem(i, per)
        t0 = pl.multiple_of(b * step, step)
        start_of_all = (me == 0) & (b == 0)
        band = jnp.where(first_col & start_of_all, 0.0, in_band).astype(BF16)
        running = dot(band, ext[pl.ds(t0, step + HALO), :])
        pos = me * tok + t0 + iota((step, 1), 0)
        inverse = 1.0 / jnp.minimum(pos + 1, window).astype(F32)
        own = ext[pl.ds(t0 + HALO, step), :].astype(F32)
        contrast = (running * inverse - own).astype(BF16)
        mixture = dot(contrast, gm_ref[0])
        pooled[pl.ds(t0, step), :] = (mixture * scale_ref[...]).astype(BF16)
        return carry

    lax.fori_loop(0, per, pool, 0)
    stage(1, lines[:1])
    locals_[1].wait()

    def partial(d, col):
        base = pl.multiple_of(lax.rem(x + d, NX) * rows, rows)
        return dot(pooled[pl.ds(base, rows), :], ow[:, pl.ds(pl.multiple_of(col, 512), 512)])

    def rs_copy(i, src, dst, d):
        return pltpu.make_async_remote_copy(
            src_ref=src, dst_ref=dst, send_sem=rs_send.at[i], recv_sem=rs_recv.at[i],
            device_id=x_peer(d), device_id_type=MESH,
        )

    lo, hi = pl.ds(0, half), pl.ds(half, half)
    plus1 = rs_copy(0, s1.at[0], r1.at[0], 1)
    minus1 = rs_copy(1, s1.at[1], r1.at[1], NX - 1)
    plus2 = rs_copy(2, s2.at[0, 0], rl.at[1], 1)
    minus2 = rs_copy(3, s2.at[1, 0], rr.at[0], NX - 1)
    plus3 = rs_copy(4, s2.at[0, 1], rl.at[0], 1)
    minus3 = rs_copy(5, s2.at[1, 1], rr.at[1], NX - 1)

    def fill(j, carry):
        col = pl.multiple_of(j * 512, 512)
        s1[0, :, pl.ds(col, 512)] = partial(2, col).astype(BF16)
        s1[1, :, pl.ds(col, 512)] = partial(2, half + col).astype(BF16)
        return carry

    lax.fori_loop(0, half // 512, fill, 0)
    plus1.start()
    minus1.start()
    stage(2, lines[1:2])
    lax.fori_loop(per, NX * per, pool, 0)

    def fill2(j, carry):
        col = pl.multiple_of(j * 512, 512)
        s2[0, 0, :, pl.ds(col, 512)] = partial(1, half + col).astype(BF16)
        s2[1, 0, :, pl.ds(col, 512)] = partial(NX - 1, col).astype(BF16)
        return carry

    lax.fori_loop(0, half // 512, fill2, 0)
    plus2.start()
    minus2.start()

    def fill3(j, carry):
        col = pl.multiple_of(j * 512, 512)
        accp[:, pl.ds(col, 512)] = partial(1, col)
        accm[:, pl.ds(col, 512)] = partial(NX - 1, half + col)
        return carry

    lax.fori_loop(0, half // 512, fill3, 0)

    def fill4(j, carry):
        col = pl.multiple_of(j * 512, 512)
        acc[:, pl.ds(col, 512)] = partial(0, col)
        return carry

    lax.fori_loop(0, width // 512, fill4, 0)
    plus1.wait_recv()
    s2[0, 1] = (accp[...] + r1[0].astype(F32)).astype(BF16)
    plus3.start()
    minus1.wait_recv()
    s2[1, 1] = (accm[...] + r1[1].astype(F32)).astype(BF16)
    minus3.start()
    weight_copy(0, 0).wait_recv()
    swap.start()

    lane16 = lax.rem(iota((rows, lanes), 1), BLK)
    tail_at = 3 * (lane16 - CAP)

    def weights_of(g, carry):
        spread = jnp.where(iota((lanes, lanes), 0) == g * 8 + iota((lanes, lanes), 1) // BLK, 1.0, 0.0)
        spread = spread.astype(BF16)
        at = dot(mtok[...], spread)
        share = dot(shr[...], spread)
        for k in range(4):
            if k < 3:
                want = jnp.where(lane16 >= CAP, tail_at + k, -5)
            else:
                want = jnp.where(lane16 < CAP, lane16, -5)
            onehot[k, g] = jnp.where(at == want.astype(F32), share, 0.0).astype(BF16)
        return carry

    lax.fori_loop(0, NZ, weights_of, 0)

    locals_[2].wait()
    plus2.wait_recv()
    minus2.wait_recv()
    plus3.wait_recv()
    minus3.wait_recv()

    def norm(b, carry):
        at = pl.ds(pl.multiple_of(b * 32, 32), 32)
        halves = []
        for h in range(2):
            cols = pl.ds(h * half, half)
            projected = acc[at, cols] + rl[h, at, :].astype(F32) + rr[h, at, :].astype(F32)
            m = (res[at, cols].astype(F32) + projected).astype(BF16)
            middle[at, cols] = m
            halves.append(m.astype(F32))
        squares = sum(jnp.sum(m * m, axis=1, keepdims=True) for m in halves)
        factor = lax.rsqrt(squares / width + 1e-06)
        for h in range(2):
            cols = pl.ds(h * half, half)
            normed[at, cols] = (halves[h] * factor * gain_ref[:, cols]).astype(BF16)
        return carry

    lax.fori_loop(0, rows // 32, norm, 0)

    def lag_of(g):
        return 4 + ((g + 1) // 2) * (1 - 2 * lax.rem(g, 2))

    gl = 8 * BLK
    row16 = lax.rem(iota((gl, rows), 0), BLK)
    sign = 1 - 2 * c

    def block(idx):
        return pl.ds(pl.multiple_of(idx * BLK, BLK), BLK)

    def place(lag, yy, cc):
        ze = lax.rem(z - lag + NZ, NZ)
        own = lag == 0
        plus = (lag < 4) | ((lag == 4) & (c == 0))
        shift = jnp.where(own, 0, jnp.where(plus, 1, NZ - 1))
        j = jnp.where(plus, lag - 1, 7 - lag)
        away = jnp.where(x // 2 == cc, 0, 1)
        core = jnp.where(own, cc, jnp.where(plus, 0, 1))
        xx = jnp.where(own | (away == 0), x, mirror)
        slot = jnp.where(
            own, y * 2 + c, jnp.where(j < 3, 8 + 16 * j + (y * 2 + c) * 2 + away, 56 + y * 2 + away)
        )
        dev = (lax.rem(ze + shift, NZ), yy, core, xx)
        return (ze * NY + yy) * NC + cc, dev, slot

    def is_me(dev):
        return (dev[0] == z) & (dev[1] == y) & (dev[2] == c) & (dev[3] == x)

    def origin(slot_group, yy, cc, away):
        if slot_group == "own":
            return (z, yy, cc, x), yy * 2 + cc, me
        j = slot_group
        zz = lax.rem(z + sign * j + NZ, NZ)
        xx = jnp.where(away == 0, x, mirror)
        slot = jnp.where(j < 3, 8 + 16 * j + (yy * 2 + cc) * 2 + away, 56 + yy * 2 + away)
        return (zz, yy, cc, xx), slot, imported

    imported = (lax.rem(z - sign + NZ, NZ) * NY + y) * NC + x // 2

    def members(group, act):
        if isinstance(group, str):
            todo = [(q // NC, q % NC, 0) for q in range(8)]
        elif isinstance(group, int):
            todo = [(q, c, away) for q in range(4) for away in range(2)]
        else:
            todo = [(q // NC, q % NC, away) for q in range(8) for away in range(2)]
        for q, cc, away in todo:
            core = cc if isinstance(group, int) else lax.rem(c + cc, NC)
            dev, slot, expert = origin(group, lax.rem(y + q, NY), core, away)
            pl.when(jnp.logical_not(is_me(dev)))(functools.partial(act, dev, slot, expert))

    def out_copy(expert, dev, slot):
        return pltpu.make_async_remote_copy(
            src_ref=send.at[block(expert), :], dst_ref=recv.at[block(slot), :],
            send_sem=d_send.at[expert], recv_sem=d_recv.at[slot],
            device_id=dev, device_id_type=MESH,
        )

    def back_copy(dev, slot, expert):
        return pltpu.make_async_remote_copy(
            src_ref=ret.at[block(slot), :], dst_ref=back.at[block(expert), :],
            send_sem=b_send.at[slot], recv_sem=b_recv.at[expert],
            device_id=dev, device_id_type=MESH,
        )

    def back_wait(expert, dev):
        return pltpu.make_async_remote_copy(
            src_ref=ret.at[block(expert), :], dst_ref=back.at[block(expert), :],
            send_sem=b_send.at[expert], recv_sem=b_recv.at[expert],
            device_id=dev, device_id_type=MESH,
        )

    def each_expert(lag, act):
        for q in range(8):
            expert, dev, slot = place(lag, lax.rem(y + q // NC, NY), lax.rem(c + q % NC, NC))
            pl.when(jnp.logical_not(is_me(dev)))(functools.partial(act, expert, dev, slot))

    def dispatch(g, carry):
        lag = lag_of(g)
        ze = lax.rem(z - lag + NZ, NZ)
        at8 = mt[pl.ds(pl.multiple_of(ze * 8, 8), 8), :]
        at = jnp.broadcast_to(at8[:, None, :], (8, BLK, rows)).reshape(gl, rows)
        main = jnp.where(at == jnp.where(row16 < CAP, row16, -5).astype(F32), 1.0, 0.0).astype(BF16)
        at_rows = pl.ds(pl.multiple_of(ze * gl, gl), gl)
        for k in range(3):
            want = jnp.where(row16 >= CAP, 3 * (row16 - CAP) + k, -5).astype(F32)
            tail = jnp.where(at == want, 1.0, 0.0).astype(BF16)
            cols = pl.ds(k * q4, q4)
            packed = dot(main, normed[:, cols]) + dot(tail, normed[:, pl.ds(3 * q4, q4)])
            send[at_rows, cols] = packed.astype(BF16)
        each_expert(lag, lambda expert, dev, slot: out_copy(expert, dev, slot).start())
        return carry

    lax.fori_loop(0, NZ, dispatch, 0)
    own_slot, far_slot = y * 2 + c, 8 + (y * 2 + c) * 2
    recv[block(own_slot), :] = send[block(me), :]
    recv[block(far_slot), :] = send[block(imported), :]
    for i in (3, 4, 5):
        locals_[i].wait()

    def ffn(group, first, count, gate_w, up_w, down_w):
        members(group, lambda dev, slot, expert: out_copy(slot, dev, slot).wait_recv())
        ra, ca = iota((count, count), 0), iota((count, count), 1)
        same = ra // BLK == ca // BLK
        r16, c16 = lax.rem(ra, BLK), lax.rem(ca, BLK)
        keep = lax.rem(iota((count, q4), 0), BLK) < CAP
        at_rows = pl.ds(pl.multiple_of(first * BLK, 128), count)
        tail = jnp.zeros((count, q4), F32)
        for k in range(3):
            pick = jnp.where(same & (c16 >= CAP) & (r16 == 3 * (c16 - CAP) + k), 1.0, 0.0)
            tail = tail + dot(pick.astype(BF16), recv[at_rows, pl.ds(k * q4, q4)])
        tail = tail.astype(BF16)
        rows_in = recv[at_rows, :]
        gate = dot(rows_in, gate_w[pl.ds(0, 3 * q4), :]) + dot(tail, gate_w[pl.ds(3 * q4, q4), :])
        up = dot(rows_in, up_w[pl.ds(0, 3 * q4), :]) + dot(tail, up_w[pl.ds(3 * q4, q4), :])
        hidden = (gate / (1.0 + jnp.exp(-gate)) * up).astype(BF16)
        last = dot(hidden, down_w[:, pl.ds(3 * q4, q4)]).astype(BF16)
        for k in range(3):
            put = jnp.where(same & (r16 >= CAP) & (c16 == 3 * (r16 - CAP) + k), 1.0, 0.0)
            cols = pl.ds(k * q4, q4)
            ret[at_rows, cols] = jnp.where(
                keep, dot(hidden, down_w[:, cols]), dot(put.astype(BF16), last)
            ).astype(BF16)
        members(group, lambda dev, slot, expert: back_copy(dev, slot, expert).start())

    ffn("own", 0, 8 * BLK, wg, wu, wd)
    back[block(me), :] = ret[block(own_slot), :]
    for i in (1, 2):
        weight_copy(i, 0).wait_recv()
    swap.wait_recv()

    def far(i, carry):
        j = jnp.where(i == 0, 0, 3 - i)
        ffn(j, 8 + 16 * j, 16 * BLK, wg2, wu2, wd2)
        return carry

    lax.fori_loop(0, 1, far, 0)
    back[block(imported), :] = ret[block(far_slot), :]
    ffn(3, 56, 8 * BLK, wg2, wu2, wd2)
    lax.fori_loop(1, 3, far, 0)

    def clear(b, carry):
        at = pl.ds(pl.multiple_of(b * 32, 32), 32)
        acc[at, :] = middle[at, :].astype(F32)
        return carry

    lax.fori_loop(0, rows // 32, clear, 0)

    def combine(g, carry):
        lag = jnp.where(g < 2, g, jnp.where(g == 2, 7, jnp.where(g == 3, 4, jnp.where(
            g < 6, 2 * g - 5, 4 * g - 22))))
        zz = lax.rem(z - lag + NZ, NZ)
        each_expert(lag, lambda expert, dev, slot: back_wait(expert, dev).wait_recv())
        at_rows = pl.ds(pl.multiple_of(zz * gl, gl), gl)
        extra = acc[:, pl.ds(3 * q4, q4)]
        for k in range(3):
            cols = pl.ds(k * q4, q4)
            piece = back[at_rows, cols]
            acc[:, cols] += dot(onehot[3, zz], piece)
            extra = extra + dot(onehot[k, zz], piece)
        acc[:, pl.ds(3 * q4, q4)] = extra
        return carry

    lax.fori_loop(0, NZ, combine, 0)

    def finish(b, carry):
        at = pl.ds(pl.multiple_of(b * 32, 32), 32)
        out_ref[at, :] = acc[at, :].astype(BF16)
        return carry

    lax.fori_loop(0, rows // 32, finish, 0)
    for cp in (plus1, minus1, plus2, minus2, plus3, minus3):
        cp.wait_send()

    def drain(g, carry):
        each_expert(g, lambda expert, dev, slot: out_copy(expert, dev, slot).wait_send())
        return carry

    lax.fori_loop(0, NZ, drain, 0)
    members("own", lambda dev, slot, expert: back_copy(dev, slot, expert).wait_send())
    members(3, lambda dev, slot, expert: back_copy(dev, slot, expert).wait_send())

    def drain_far(j, carry):
        members(j, lambda dev, slot, expert: back_copy(dev, slot, expert).wait_send())
        return carry

    lax.fori_loop(0, 3, drain_far, 0)

    halo.wait_send()
    swap.wait_send()

    @pl.when(gives)
    def _():
        for i in range(3):
            for side in range(2):
                weight_copy(i, side).wait_send()


def body(
    pooled_in, group_map, pool_scale, out_weight, residual, norm_gain,
    gate_weight, up_weight, down_weight, route_expert, route_score,
):
    tok, ch = pooled_in.shape
    rows, width = residual.shape
    ff = gate_weight.shape[2]
    half = width // 2
    packed = (NSP * BLK, 3 * width // 4)
    vmem = pl.BlockSpec(memory_space=pltpu.VMEM)
    hbm = pl.BlockSpec(memory_space=pl.ANY)
    dma = pltpu.SemaphoreType.DMA
    return pl.pallas_call(
        kernel,
        out_shape=jax.ShapeDtypeStruct((rows, width), BF16),
        in_specs=[hbm, vmem, vmem, hbm, hbm, vmem, hbm, hbm, hbm, vmem, vmem],
        out_specs=vmem,
        scratch_shapes=[
            pltpu.VMEM((HALO + tok, ch), BF16),
            pltpu.VMEM((ch, width), BF16),
            pltpu.VMEM((rows, width), BF16),
            pltpu.VMEM((width, ff), BF16),
            pltpu.VMEM((width, ff), BF16),
            pltpu.VMEM((ff, width), BF16),
            pltpu.VMEM((width, ff), BF16),
            pltpu.VMEM((width, ff), BF16),
            pltpu.VMEM((ff, width), BF16),
            pltpu.VMEM((tok, ch), BF16),
            pltpu.VMEM((2, rows, half), BF16),
            pltpu.VMEM((2, 2, rows, half), BF16),
            pltpu.VMEM((2, rows, half), BF16),
            pltpu.VMEM((2, rows, half), BF16),
            pltpu.VMEM((2, rows, half), BF16),
            pltpu.VMEM((rows, half), F32),
            pltpu.VMEM((rows, half), F32),
            pltpu.VMEM((rows, width), F32),
            pltpu.VMEM((rows, width), BF16),
            pltpu.VMEM((rows, width), BF16),
            pltpu.VMEM((128, rows), F32),
            pltpu.VMEM((rows, 128), BF16),
            pltpu.VMEM((rows, 128), BF16),
            pltpu.VMEM((4, NZ, rows, 128), BF16),
            pltpu.VMEM(packed, BF16),
            pltpu.VMEM(packed, BF16),
            pltpu.VMEM(packed, BF16),
            pltpu.VMEM(packed, BF16),
            dma((6,)),
            pltpu.SemaphoreType.REGULAR((3,)),
            dma((2,)),
            dma((2,)),
            dma((6,)),
            dma((3,)),
            dma((6,)),
            dma((6,)),
            dma((NSP,)),
            dma((NSP,)),
            dma((NSP,)),
            dma((NSP,)),
        ],
        compiler_params=pltpu.CompilerParams(
            collective_id=0, has_side_effects=True, vmem_limit_bytes=60 * 2**20
        ),
    )(
        pooled_in, group_map, pool_scale.reshape(1, -1), out_weight, residual,
        norm_gain.reshape(1, -1), gate_weight.reshape(width, ff), up_weight.reshape(width, ff),
        down_weight.reshape(ff, width), route_expert.T, route_score.T,
    )


def solution(mesh):
    split = Mesh(mesh.devices.reshape(NZ, NY, NC, NX), AXES)
    sp_tp = AXES
    in_specs = (
        P(SP, "x"),
        P("x", None, None),
        P("x"),
        P("x", None),
        P(sp_tp, None),
        P(),
        P(SP, None, None),
        P(SP, None, None),
        P(SP, None, None),
        P(sp_tp, None),
        P(sp_tp, None),
    )
    return jax.shard_map(
        body, mesh=split, in_specs=in_specs, out_specs=P(sp_tp, None), check_vma=False
    )
```

```python
import functools

import jax
import jax.numpy as jnp
from jax import lax
from jax.experimental import pallas as pl
from jax.experimental.pallas import tpu as pltpu
from jax.sharding import Mesh
from jax.sharding import PartitionSpec as P

AXES = ("z", "y", "c", "x")
SP = ("z", "y", "c")
MESH = pl.DeviceIdType.MESH
NZ, NY, NC, NX = 8, 4, 2, 4
NSP = NZ * NY * NC
HALO = 16
CAP = 12
BLK = 16
F32, BF16 = jnp.float32, jnp.bfloat16


def dot(a, b):
    return jnp.dot(a, b, preferred_element_type=F32)


def iota(shape, dim):
    return lax.broadcasted_iota(jnp.int32, shape, dim)


def kernel(
    pin_hbm, gm_ref, scale_ref, ow_hbm, res_hbm, gain_ref, wg_hbm, wu_hbm, wd_hbm, re_ref, sc_ref,
    out_ref,
    ext, ow, res, wg, wu, wd, wg2, wu2, wd2, pooled,
    s1, s2, r1, rl, rr, accp, accm, acc, middle, normed,
    mt, mtok, shr, onehot,
    send, recv, ret, back,
    lsem, gate_sem, halo_sem, swap_sem, w_send, w_recv, rs_send, rs_recv, d_send, d_recv, b_send, b_recv,
):
    z, y, c, x = (lax.axis_index(a) for a in AXES)
    me = (z * NY + y) * NC + c
    rows = res_hbm.shape[0]
    width = res_hbm.shape[1]
    tok = pin_hbm.shape[0]
    half = width // 2
    q4 = width // 4

    def sp_peer(idx, xx=x):
        return (idx // (NY * NC), (idx // NC) % NY, idx % NC, xx)

    mirror = NX - 1 - x

    def x_peer(d):
        return (z, y, c, lax.rem(x + d, NX))

    barrier = pltpu.get_barrier_semaphore()

    lines = [(z, y, 1 - c, x), (z, y, c, mirror), (z, y, c, x + 1 - 2 * lax.rem(x, 2))]
    y_line = [(z, lax.rem(y + k, NY), c, x) for k in range(1, NY)]
    lines += y_line + [(lax.rem(z + k, NZ), y, c, x) for k in range(1, NZ)]
    lines.append(sp_peer(lax.rem(me + 2 * c - 1 + NSP, NSP)))
    lines += [(lax.rem(z + k, NZ), y, 1 - c, x) for k in (1, NZ - 1)]
    for dev in lines:
        pl.semaphore_signal(barrier, inc=1, device_id=dev, device_id_type=MESH)

    def stage(i, devs):
        for dev in devs:
            pl.semaphore_signal(gate_sem.at[i], inc=1, device_id=dev, device_id_type=MESH)
        pl.semaphore_wait(gate_sem.at[i], len(devs))

    locals_ = [
        pltpu.make_async_copy(src, dst, lsem.at[i])
        for i, (src, dst) in enumerate(
            (
                (pin_hbm, ext.at[pl.ds(HALO, tok), :]),
                (ow_hbm, ow),
                (res_hbm, res),
                (wg_hbm, wg),
                (wu_hbm, wu),
                (wd_hbm, wd),
            )
        )
    ]
    for cp in locals_:
        cp.start()
    pl.semaphore_wait(barrier, len(lines))

    halo = pltpu.make_async_remote_copy(
        src_ref=pin_hbm.at[pl.ds(tok - HALO, HALO), :],
        dst_ref=ext.at[pl.ds(0, HALO), :],
        send_sem=halo_sem.at[0],
        recv_sem=halo_sem.at[1],
        device_id=sp_peer(lax.rem(me + 1, NSP)),
        device_id_type=MESH,
    )
    halo.start()

    gives = c == x // 2

    mid = wd_hbm.shape[0] // 2
    pair = x + 1 - 2 * lax.rem(x, 2)

    def my_half(ref):
        return ref.at[pl.ds(pl.multiple_of(lax.rem(x, 2) * mid, mid), mid), :]

    def weight_copy(i, side):
        src = (my_half(wd_hbm), wg_hbm, wu_hbm)[i]
        dst = (my_half(wd2), wg2, wu2)[i]
        return pltpu.make_async_remote_copy(
            src_ref=src, dst_ref=dst, send_sem=w_send.at[2 * i + side], recv_sem=w_recv.at[i],
            device_id=(lax.rem(z + (1, NZ - 1)[side], NZ), y, side, x), device_id_type=MESH,
        )

    swap = pltpu.make_async_remote_copy(
        src_ref=my_half(wd2), dst_ref=my_half(wd2), send_sem=swap_sem.at[0], recv_sem=swap_sem.at[1],
        device_id=(z, y, c, pair), device_id_type=MESH,
    )

    @pl.when(gives)
    def _():
        for i in range(3):
            for side in range(2):
                weight_copy(i, side).start()

    window = jnp.left_shift(jnp.int32(2), x)
    step = 128
    lag = iota((step, step + HALO), 0) + HALO - iota((step, step + HALO), 1)
    in_band = jnp.where((lag >= 0) & (lag < window), 1.0, 0.0)
    first_col = iota((step, step + HALO), 1) < HALO

    locals_[0].wait()
    pl.when(x == 2)(halo.wait_recv)

    per = rows // step

    def pool(i, carry):
        part = i // per
        d = jnp.where(part == 0, 2, jnp.where(part == 3, 0, 2 * part - 1))
        b = lax.rem(x + d, NX) * per + lax.rem(i, per)
        t0 = pl.multiple_of(b * step, step)
        start_of_all = (me == 0) & (b == 0)
        band = jnp.where(first_col & start_of_all, 0.0, in_band).astype(BF16)
        running = dot(band, ext[pl.ds(t0, step + HALO), :])
        pos = me * tok + t0 + iota((step, 1), 0)
        inverse = 1.0 / jnp.minimum(pos + 1, window).astype(F32)
        own = ext[pl.ds(t0 + HALO, step), :].astype(F32)
        contrast = (running * inverse - own).astype(BF16)
        mixture = dot(contrast, gm_ref[0])
        pooled[pl.ds(t0, step), :] = (mixture * scale_ref[...]).astype(BF16)
        return carry

    lax.fori_loop(0, per, pool, 0)
    locals_[1].wait()

    def partial(d, col):
        base = pl.multiple_of(lax.rem(x + d, NX) * rows, rows)
        return dot(pooled[pl.ds(base, rows), :], ow[:, pl.ds(pl.multiple_of(col, 512), 512)])

    def rs_copy(i, src, dst, d):
        return pltpu.make_async_remote_copy(
            src_ref=src, dst_ref=dst, send_sem=rs_send.at[i], recv_sem=rs_recv.at[i],
            device_id=x_peer(d), device_id_type=MESH,
        )

    lo, hi = pl.ds(0, half), pl.ds(half, half)
    plus1 = rs_copy(0, s1.at[0], r1.at[0], 1)
    minus1 = rs_copy(1, s1.at[1], r1.at[1], NX - 1)
    plus2 = rs_copy(2, s2.at[0, 0], rl.at[1], 1)
    minus2 = rs_copy(3, s2.at[1, 0], rr.at[0], NX - 1)
    plus3 = rs_copy(4, s2.at[0, 1], rl.at[0], 1)
    minus3 = rs_copy(5, s2.at[1, 1], rr.at[1], NX - 1)

    def fill(j, carry):
        col = pl.multiple_of(j * 512, 512)
        s1[0, :, pl.ds(col, 512)] = partial(2, col).astype(BF16)
        s1[1, :, pl.ds(col, 512)] = partial(2, half + col).astype(BF16)
        return carry

    lax.fori_loop(0, half // 512, fill, 0)
    plus1.start()
    minus1.start()
    pl.when(x != 2)(halo.wait_recv)
    lax.fori_loop(per, NX * per, pool, 0)

    def fill2(j, carry):
        col = pl.multiple_of(j * 512, 512)
        s2[0, 0, :, pl.ds(col, 512)] = partial(1, half + col).astype(BF16)
        s2[1, 0, :, pl.ds(col, 512)] = partial(NX - 1, col).astype(BF16)
        return carry

    lax.fori_loop(0, half // 512, fill2, 0)
    plus2.start()
    minus2.start()
    stage(0, y_line)

    def fill3(j, carry):
        col = pl.multiple_of(j * 512, 512)
        accp[:, pl.ds(col, 512)] = partial(1, col)
        accm[:, pl.ds(col, 512)] = partial(NX - 1, half + col)
        return carry

    lax.fori_loop(0, half // 512, fill3, 0)

    def fill4(j, carry):
        col = pl.multiple_of(j * 512, 512)
        acc[:, pl.ds(col, 512)] = partial(0, col)
        return carry

    lax.fori_loop(0, width // 512, fill4, 0)
    stage(1, lines[:1])

    lanes = 128
    el = iota((rows, lanes), 1)
    mt[...] = jnp.zeros((lanes, rows), F32)
    mt[0:2, :] = re_ref[...].astype(F32)
    mt[2:4, :] = sc_ref[...]
    by_token = jnp.transpose(mt[...])
    el_f = el.astype(F32)
    named0 = by_token[:, 0:1] == el_f
    named1 = by_token[:, 1:2] == el_f
    named = jnp.where(named0 | named1, 1.0, 0.0)
    before = jnp.where(iota((rows, rows), 1) < iota((rows, rows), 0), 1.0, 0.0).astype(BF16)
    rank = dot(before, named.astype(BF16))
    slot = jnp.where(named > 0.5, rank, -1.0)
    mtok[...] = slot.astype(BF16)
    mt[...] = jnp.transpose(slot)
    s0 = by_token[:, 2:3]
    s1v = by_token[:, 3:4]
    total = s0 + s1v
    shr[...] = (
        jnp.where(named0, s0 / total, 0.0) + jnp.where(named1, s1v / total, 0.0)
    ).astype(BF16)

    plus1.wait_recv()
    s2[0, 1] = (accp[...] + r1[0].astype(F32)).astype(BF16)
    plus3.start()
    minus1.wait_recv()
    s2[1, 1] = (accm[...] + r1[1].astype(F32)).astype(BF16)
    minus3.start()
    weight_copy(0, 0).wait_recv()
    swap.start()
    stage(2, lines[1:2])

    lane16 = lax.rem(iota((rows, lanes), 1), BLK)
    tail_at = 3 * (lane16 - CAP)

    def weights_of(g, carry):
        spread = jnp.where(iota((lanes, lanes), 0) == g * 8 + iota((lanes, lanes), 1) // BLK, 1.0, 0.0)
        spread = spread.astype(BF16)
        at = dot(mtok[...], spread)
        share = dot(shr[...], spread)
        for k in range(4):
            if k < 3:
                want = jnp.where(lane16 >= CAP, tail_at + k, -5)
            else:
                want = jnp.where(lane16 < CAP, lane16, -5)
            onehot[k, g] = jnp.where(at == want.astype(F32), share, 0.0).astype(BF16)
        return carry

    lax.fori_loop(0, NZ, weights_of, 0)

    locals_[2].wait()
    plus2.wait_recv()
    minus2.wait_recv()
    plus3.wait_recv()
    minus3.wait_recv()

    def norm(b, carry):
        at = pl.ds(pl.multiple_of(b * 32, 32), 32)
        halves = []
        for h in range(2):
            cols = pl.ds(h * half, half)
            projected = acc[at, cols] + rl[h, at, :].astype(F32) + rr[h, at, :].astype(F32)
            m = (res[at, cols].astype(F32) + projected).astype(BF16)
            middle[at, cols] = m
            halves.append(m.astype(F32))
        squares = sum(jnp.sum(m * m, axis=1, keepdims=True) for m in halves)
        factor = lax.rsqrt(squares / width + 1e-06)
        for h in range(2):
            cols = pl.ds(h * half, half)
            normed[at, cols] = (halves[h] * factor * gain_ref[:, cols]).astype(BF16)
        return carry

    lax.fori_loop(0, rows // 32, norm, 0)

    def lag_of(g):
        return 4 + ((g + 1) // 2) * (1 - 2 * lax.rem(g, 2))

    gl = 8 * BLK
    row16 = lax.rem(iota((gl, rows), 0), BLK)
    sign = 1 - 2 * c

    def block(idx):
        return pl.ds(pl.multiple_of(idx * BLK, BLK), BLK)

    def place(lag, yy, cc):
        ze = lax.rem(z - lag + NZ, NZ)
        own = lag == 0
        plus = (lag < 4) | ((lag == 4) & (c == 0))
        shift = jnp.where(own, 0, jnp.where(plus, 1, NZ - 1))
        j = jnp.where(plus, lag - 1, 7 - lag)
        away = jnp.where(x // 2 == cc, 0, 1)
        core = jnp.where(own, cc, jnp.where(plus, 0, 1))
        xx = jnp.where(own | (away == 0), x, mirror)
        slot = jnp.where(
            own, y * 2 + c, jnp.where(j < 3, 8 + 16 * j + (y * 2 + c) * 2 + away, 56 + y * 2 + away)
        )
        dev = (lax.rem(ze + shift, NZ), yy, core, xx)
        return (ze * NY + yy) * NC + cc, dev, slot

    def is_me(dev):
        return (dev[0] == z) & (dev[1] == y) & (dev[2] == c) & (dev[3] == x)

    def origin(slot_group, yy, cc, away):
        if slot_group == "own":
            return (z, yy, cc, x), yy * 2 + cc, me
        j = slot_group
        zz = lax.rem(z + sign * j + NZ, NZ)
        xx = jnp.where(away == 0, x, mirror)
        slot = jnp.where(j < 3, 8 + 16 * j + (yy * 2 + cc) * 2 + away, 56 + yy * 2 + away)
        return (zz, yy, cc, xx), slot, imported

    imported = (lax.rem(z - sign + NZ, NZ) * NY + y) * NC + x // 2

    def members(group, act):
        if isinstance(group, str):
            todo = [(q // NC, q % NC, 0) for q in range(8)]
        elif isinstance(group, int):
            todo = [(q, c, away) for q in range(4) for away in range(2)]
        else:
            todo = [(q // NC, q % NC, away) for q in range(8) for away in range(2)]
        for q, cc, away in todo:
            core = cc if isinstance(group, int) else lax.rem(c + cc, NC)
            dev, slot, expert = origin(group, lax.rem(y + q, NY), core, away)
            pl.when(jnp.logical_not(is_me(dev)))(functools.partial(act, dev, slot, expert))

    def out_copy(expert, dev, slot):
        return pltpu.make_async_remote_copy(
            src_ref=send.at[block(expert), :], dst_ref=recv.at[block(slot), :],
            send_sem=d_send.at[expert], recv_sem=d_recv.at[slot],
            device_id=dev, device_id_type=MESH,
        )

    def back_copy(dev, slot, expert):
        return pltpu.make_async_remote_copy(
            src_ref=ret.at[block(slot), :], dst_ref=back.at[block(expert), :],
            send_sem=b_send.at[slot], recv_sem=b_recv.at[expert],
            device_id=dev, device_id_type=MESH,
        )

    def back_wait(expert, dev):
        return pltpu.make_async_remote_copy(
            src_ref=ret.at[block(expert), :], dst_ref=back.at[block(expert), :],
            send_sem=b_send.at[expert], recv_sem=b_recv.at[expert],
            device_id=dev, device_id_type=MESH,
        )

    def each_expert(lag, act):
        for q in range(8):
            expert, dev, slot = place(lag, lax.rem(y + q // NC, NY), lax.rem(c + q % NC, NC))
            pl.when(jnp.logical_not(is_me(dev)))(functools.partial(act, expert, dev, slot))

    def dispatch(g, carry):
        lag = lag_of(g)
        ze = lax.rem(z - lag + NZ, NZ)
        at8 = mt[pl.ds(pl.multiple_of(ze * 8, 8), 8), :]
        at = jnp.broadcast_to(at8[:, None, :], (8, BLK, rows)).reshape(gl, rows)
        main = jnp.where(at == jnp.where(row16 < CAP, row16, -5).astype(F32), 1.0, 0.0).astype(BF16)
        at_rows = pl.ds(pl.multiple_of(ze * gl, gl), gl)
        for k in range(3):
            want = jnp.where(row16 >= CAP, 3 * (row16 - CAP) + k, -5).astype(F32)
            tail = jnp.where(at == want, 1.0, 0.0).astype(BF16)
            cols = pl.ds(k * q4, q4)
            packed = dot(main, normed[:, cols]) + dot(tail, normed[:, pl.ds(3 * q4, q4)])
            send[at_rows, cols] = packed.astype(BF16)
        each_expert(lag, lambda expert, dev, slot: out_copy(expert, dev, slot).start())
        return carry

    lax.fori_loop(0, NZ, dispatch, 0)
    own_slot, far_slot = y * 2 + c, 8 + (y * 2 + c) * 2
    recv[block(own_slot), :] = send[block(me), :]
    recv[block(far_slot), :] = send[block(imported), :]
    for i in (3, 4, 5):
        locals_[i].wait()

    def ffn(group, first, count, gate_w, up_w, down_w):
        members(group, lambda dev, slot, expert: out_copy(slot, dev, slot).wait_recv())
        ra, ca = iota((count, count), 0), iota((count, count), 1)
        same = ra // BLK == ca // BLK
        r16, c16 = lax.rem(ra, BLK), lax.rem(ca, BLK)
        keep = lax.rem(iota((count, q4), 0), BLK) < CAP
        at_rows = pl.ds(pl.multiple_of(first * BLK, 128), count)
        tail = jnp.zeros((count, q4), F32)
        for k in range(3):
            pick = jnp.where(same & (c16 >= CAP) & (r16 == 3 * (c16 - CAP) + k), 1.0, 0.0)
            tail = tail + dot(pick.astype(BF16), recv[at_rows, pl.ds(k * q4, q4)])
        tail = tail.astype(BF16)
        rows_in = recv[at_rows, :]
        gate = dot(rows_in, gate_w[pl.ds(0, 3 * q4), :]) + dot(tail, gate_w[pl.ds(3 * q4, q4), :])
        up = dot(rows_in, up_w[pl.ds(0, 3 * q4), :]) + dot(tail, up_w[pl.ds(3 * q4, q4), :])
        hidden = (gate / (1.0 + jnp.exp(-gate)) * up).astype(BF16)
        last = dot(hidden, down_w[:, pl.ds(3 * q4, q4)]).astype(BF16)
        for k in range(3):
            put = jnp.where(same & (r16 >= CAP) & (c16 == 3 * (r16 - CAP) + k), 1.0, 0.0)
            cols = pl.ds(k * q4, q4)
            ret[at_rows, cols] = jnp.where(
                keep, dot(hidden, down_w[:, cols]), dot(put.astype(BF16), last)
            ).astype(BF16)
        members(group, lambda dev, slot, expert: back_copy(dev, slot, expert).start())

    ffn("own", 0, 8 * BLK, wg, wu, wd)
    back[block(me), :] = ret[block(own_slot), :]
    for i in (1, 2):
        weight_copy(i, 0).wait_recv()
    swap.wait_recv()

    def far(i, carry):
        j = jnp.where(i == 0, 0, 3 - i)
        ffn(j, 8 + 16 * j, 16 * BLK, wg2, wu2, wd2)
        return carry

    lax.fori_loop(0, 1, far, 0)
    back[block(imported), :] = ret[block(far_slot), :]
    ffn(3, 56, 8 * BLK, wg2, wu2, wd2)
    lax.fori_loop(1, 3, far, 0)

    def clear(b, carry):
        at = pl.ds(pl.multiple_of(b * 32, 32), 32)
        acc[at, :] = middle[at, :].astype(F32)
        return carry

    lax.fori_loop(0, rows // 32, clear, 0)

    def combine(g, carry):
        lag = jnp.where(g < 2, g, jnp.where(g == 2, 7, jnp.where(g == 3, 4, jnp.where(
            g < 6, 2 * g - 5, 4 * g - 22))))
        zz = lax.rem(z - lag + NZ, NZ)
        each_expert(lag, lambda expert, dev, slot: back_wait(expert, dev).wait_recv())
        at_rows = pl.ds(pl.multiple_of(zz * gl, gl), gl)
        extra = acc[:, pl.ds(3 * q4, q4)]
        for k in range(3):
            cols = pl.ds(k * q4, q4)
            piece = back[at_rows, cols]
            acc[:, cols] += dot(onehot[3, zz], piece)
            extra = extra + dot(onehot[k, zz], piece)
        acc[:, pl.ds(3 * q4, q4)] = extra
        return carry

    lax.fori_loop(0, NZ, combine, 0)

    def finish(b, carry):
        at = pl.ds(pl.multiple_of(b * 32, 32), 32)
        out_ref[at, :] = acc[at, :].astype(BF16)
        return carry

    lax.fori_loop(0, rows // 32, finish, 0)
    for cp in (plus1, minus1, plus2, minus2, plus3, minus3):
        cp.wait_send()

    def drain(g, carry):
        each_expert(g, lambda expert, dev, slot: out_copy(expert, dev, slot).wait_send())
        return carry

    lax.fori_loop(0, NZ, drain, 0)
    members("own", lambda dev, slot, expert: back_copy(dev, slot, expert).wait_send())
    members(3, lambda dev, slot, expert: back_copy(dev, slot, expert).wait_send())

    def drain_far(j, carry):
        members(j, lambda dev, slot, expert: back_copy(dev, slot, expert).wait_send())
        return carry

    lax.fori_loop(0, 3, drain_far, 0)

    halo.wait_send()
    swap.wait_send()

    @pl.when(gives)
    def _():
        for i in range(3):
            for side in range(2):
                weight_copy(i, side).wait_send()


def body(
    pooled_in, group_map, pool_scale, out_weight, residual, norm_gain,
    gate_weight, up_weight, down_weight, route_expert, route_score,
):
    tok, ch = pooled_in.shape
    rows, width = residual.shape
    ff = gate_weight.shape[2]
    half = width // 2
    packed = (NSP * BLK, 3 * width // 4)
    vmem = pl.BlockSpec(memory_space=pltpu.VMEM)
    hbm = pl.BlockSpec(memory_space=pl.ANY)
    dma = pltpu.SemaphoreType.DMA
    return pl.pallas_call(
        kernel,
        out_shape=jax.ShapeDtypeStruct((rows, width), BF16),
        in_specs=[hbm, vmem, vmem, hbm, hbm, vmem, hbm, hbm, hbm, vmem, vmem],
        out_specs=vmem,
        scratch_shapes=[
            pltpu.VMEM((HALO + tok, ch), BF16),
            pltpu.VMEM((ch, width), BF16),
            pltpu.VMEM((rows, width), BF16),
            pltpu.VMEM((width, ff), BF16),
            pltpu.VMEM((width, ff), BF16),
            pltpu.VMEM((ff, width), BF16),
            pltpu.VMEM((width, ff), BF16),
            pltpu.VMEM((width, ff), BF16),
            pltpu.VMEM((ff, width), BF16),
            pltpu.VMEM((tok, ch), BF16),
            pltpu.VMEM((2, rows, half), BF16),
            pltpu.VMEM((2, 2, rows, half), BF16),
            pltpu.VMEM((2, rows, half), BF16),
            pltpu.VMEM((2, rows, half), BF16),
            pltpu.VMEM((2, rows, half), BF16),
            pltpu.VMEM((rows, half), F32),
            pltpu.VMEM((rows, half), F32),
            pltpu.VMEM((rows, width), F32),
            pltpu.VMEM((rows, width), BF16),
            pltpu.VMEM((rows, width), BF16),
            pltpu.VMEM((128, rows), F32),
            pltpu.VMEM((rows, 128), BF16),
            pltpu.VMEM((rows, 128), BF16),
            pltpu.VMEM((4, NZ, rows, 128), BF16),
            pltpu.VMEM(packed, BF16),
            pltpu.VMEM(packed, BF16),
            pltpu.VMEM(packed, BF16),
            pltpu.VMEM(packed, BF16),
            dma((6,)),
            pltpu.SemaphoreType.REGULAR((3,)),
            dma((2,)),
            dma((2,)),
            dma((6,)),
            dma((3,)),
            dma((6,)),
            dma((6,)),
            dma((NSP,)),
            dma((NSP,)),
            dma((NSP,)),
            dma((NSP,)),
        ],
        compiler_params=pltpu.CompilerParams(
            collective_id=0, has_side_effects=True, vmem_limit_bytes=60 * 2**20
        ),
    )(
        pooled_in, group_map, pool_scale.reshape(1, -1), out_weight, residual,
        norm_gain.reshape(1, -1), gate_weight.reshape(width, ff), up_weight.reshape(width, ff),
        down_weight.reshape(ff, width), route_expert.T, route_score.T,
    )


def solution(mesh):
    split = Mesh(mesh.devices.reshape(NZ, NY, NC, NX), AXES)
    sp_tp = AXES
    in_specs = (
        P(SP, "x"),
        P("x", None, None),
        P("x"),
        P("x", None),
        P(sp_tp, None),
        P(),
        P(SP, None, None),
        P(SP, None, None),
        P(SP, None, None),
        P(sp_tp, None),
        P(sp_tp, None),
    )
    return jax.shard_map(
        body, mesh=split, in_specs=in_specs, out_specs=P(sp_tp, None), check_vma=False
    )
```

```python
import functools

import jax
import jax.numpy as jnp
from jax import lax
from jax.experimental import pallas as pl
from jax.experimental.pallas import tpu as pltpu
from jax.sharding import Mesh
from jax.sharding import PartitionSpec as P

AXES = ("z", "y", "c", "x")
SP = ("z", "y", "c")
MESH = pl.DeviceIdType.MESH
NZ, NY, NC, NX = 8, 4, 2, 4
NSP = NZ * NY * NC
HALO = 16
CAP = 12
BLK = 16
F32, BF16 = jnp.float32, jnp.bfloat16


def dot(a, b):
    return jnp.dot(a, b, preferred_element_type=F32)


def iota(shape, dim):
    return lax.broadcasted_iota(jnp.int32, shape, dim)


def kernel(
    pin_hbm, gm_ref, scale_ref, ow_hbm, res_hbm, gain_ref, wg_hbm, wu_hbm, wd_hbm, re_ref, sc_ref,
    out_ref,
    ext, ow, res, wg, wu, wd, wg2, wu2, wd2, pooled,
    s1, s2, r1, rl, rr, accp, accm, acc, middle, normed,
    mt, mtok, shr, onehot,
    send, recv, ret, back,
    lsem, gate_sem, halo_sem, swap_sem, w_send, w_recv, rs_send, rs_recv, d_send, d_recv, b_send, b_recv,
):
    z, y, c, x = (lax.axis_index(a) for a in AXES)
    me = (z * NY + y) * NC + c
    rows = res_hbm.shape[0]
    width = res_hbm.shape[1]
    tok = pin_hbm.shape[0]
    half = width // 2
    q4 = width // 4

    def sp_peer(idx, xx=x):
        return (idx // (NY * NC), (idx // NC) % NY, idx % NC, xx)

    mirror = NX - 1 - x

    def x_peer(d):
        return (z, y, c, lax.rem(x + d, NX))

    barrier = pltpu.get_barrier_semaphore()

    lines = [(z, y, 1 - c, x), (z, y, c, mirror), (z, y, c, x + 1 - 2 * lax.rem(x, 2))]
    y_line = [(z, lax.rem(y + k, NY), c, x) for k in range(1, NY)]
    lines += y_line + [(lax.rem(z + k, NZ), y, c, x) for k in range(1, NZ)]
    lines.append(sp_peer(lax.rem(me + 2 * c - 1 + NSP, NSP)))
    lines += [(lax.rem(z + k, NZ), y, 1 - c, x) for k in (1, NZ - 1)]
    for dev in lines:
        pl.semaphore_signal(barrier, inc=1, device_id=dev, device_id_type=MESH)

    def stage(i, devs):
        for dev in devs:
            pl.semaphore_signal(gate_sem.at[i], inc=1, device_id=dev, device_id_type=MESH)
        pl.semaphore_wait(gate_sem.at[i], len(devs))

    locals_ = [
        pltpu.make_async_copy(src, dst, lsem.at[i])
        for i, (src, dst) in enumerate(
            (
                (pin_hbm, ext.at[pl.ds(HALO, tok), :]),
                (ow_hbm, ow),
                (res_hbm, res),
                (wg_hbm, wg),
                (wu_hbm, wu),
                (wd_hbm, wd),
            )
        )
    ]
    for cp in locals_:
        cp.start()
    pl.semaphore_wait(barrier, len(lines))

    halo = pltpu.make_async_remote_copy(
        src_ref=pin_hbm.at[pl.ds(tok - HALO, HALO), :],
        dst_ref=ext.at[pl.ds(0, HALO), :],
        send_sem=halo_sem.at[0],
        recv_sem=halo_sem.at[1],
        device_id=sp_peer(lax.rem(me + 1, NSP)),
        device_id_type=MESH,
    )
    halo.start()

    gives = c == x // 2

    mid = wd_hbm.shape[0] // 2
    pair = x + 1 - 2 * lax.rem(x, 2)

    share = 3 * wu_hbm.shape[0] // 8
    rest = pl.ds(2 * share, wu_hbm.shape[0] - 2 * share)

    def mine(ref, count):
        return ref.at[pl.ds(pl.multiple_of(lax.rem(x, 2) * count, count), count), :]

    def weight_copy(i, side):
        src = (mine(wd_hbm, mid), mine(wu_hbm, share), wg_hbm, wu_hbm.at[rest, :])[i]
        dst = (mine(wd2, mid), mine(wu2, share), wg2, wu2.at[rest, :])[i]
        return pltpu.make_async_remote_copy(
            src_ref=src, dst_ref=dst, send_sem=w_send.at[2 * i + side], recv_sem=w_recv.at[i],
            device_id=(lax.rem(z + (1, NZ - 1)[side], NZ), y, side, x), device_id_type=MESH,
        )

    swaps = [
        pltpu.make_async_remote_copy(
            src_ref=part, dst_ref=part, send_sem=swap_sem.at[2 * i], recv_sem=swap_sem.at[2 * i + 1],
            device_id=(z, y, c, pair), device_id_type=MESH,
        )
        for i, part in enumerate((mine(wd2, mid), mine(wu2, share)))
    ]

    @pl.when(gives)
    def _():
        for i in range(4):
            for side in range(2):
                weight_copy(i, side).start()

    window = jnp.left_shift(jnp.int32(2), x)
    step = 128
    lag = iota((step, step + HALO), 0) + HALO - iota((step, step + HALO), 1)
    in_band = jnp.where((lag >= 0) & (lag < window), 1.0, 0.0)
    first_col = iota((step, step + HALO), 1) < HALO

    locals_[0].wait()
    pl.when(x == 2)(halo.wait_recv)

    per = rows // step

    def pool(i, carry):
        part = i // per
        d = jnp.where(part == 0, 2, jnp.where(part == 3, 0, 2 * part - 1))
        b = lax.rem(x + d, NX) * per + lax.rem(i, per)
        t0 = pl.multiple_of(b * step, step)
        start_of_all = (me == 0) & (b == 0)
        band = jnp.where(first_col & start_of_all, 0.0, in_band).astype(BF16)
        running = dot(band, ext[pl.ds(t0, step + HALO), :])
        pos = me * tok + t0 + iota((step, 1), 0)
        inverse = 1.0 / jnp.minimum(pos + 1, window).astype(F32)
        own = ext[pl.ds(t0 + HALO, step), :].astype(F32)
        contrast = (running * inverse - own).astype(BF16)
        mixture = dot(contrast, gm_ref[0])
        pooled[pl.ds(t0, step), :] = (mixture * scale_ref[...]).astype(BF16)
        return carry

    lax.fori_loop(0, per, pool, 0)
    locals_[1].wait()

    def partial(d, col):
        base = pl.multiple_of(lax.rem(x + d, NX) * rows, rows)
        return dot(pooled[pl.ds(base, rows), :], ow[:, pl.ds(pl.multiple_of(col, 512), 512)])

    def rs_copy(i, src, dst, d):
        return pltpu.make_async_remote_copy(
            src_ref=src, dst_ref=dst, send_sem=rs_send.at[i], recv_sem=rs_recv.at[i],
            device_id=x_peer(d), device_id_type=MESH,
        )

    lo, hi = pl.ds(0, half), pl.ds(half, half)
    plus1 = rs_copy(0, s1.at[0], r1.at[0], 1)
    minus1 = rs_copy(1, s1.at[1], r1.at[1], NX - 1)
    plus2 = rs_copy(2, s2.at[0, 0], rl.at[1], 1)
    minus2 = rs_copy(3, s2.at[1, 0], rr.at[0], NX - 1)
    plus3 = rs_copy(4, s2.at[0, 1], rl.at[0], 1)
    minus3 = rs_copy(5, s2.at[1, 1], rr.at[1], NX - 1)

    def fill(j, carry):
        col = pl.multiple_of(j * 512, 512)
        s1[0, :, pl.ds(col, 512)] = partial(2, col).astype(BF16)
        s1[1, :, pl.ds(col, 512)] = partial(2, half + col).astype(BF16)
        return carry

    lax.fori_loop(0, half // 512, fill, 0)
    plus1.start()
    minus1.start()
    pl.when(x != 2)(halo.wait_recv)
    lax.fori_loop(per, NX * per, pool, 0)

    def fill2(j, carry):
        col = pl.multiple_of(j * 512, 512)
        s2[0, 0, :, pl.ds(col, 512)] = partial(1, half + col).astype(BF16)
        s2[1, 0, :, pl.ds(col, 512)] = partial(NX - 1, col).astype(BF16)
        return carry

    lax.fori_loop(0, half // 512, fill2, 0)
    plus2.start()
    minus2.start()
    stage(0, y_line)

    def fill3(j, carry):
        col = pl.multiple_of(j * 512, 512)
        accp[:, pl.ds(col, 512)] = partial(1, col)
        accm[:, pl.ds(col, 512)] = partial(NX - 1, half + col)
        return carry

    lax.fori_loop(0, half // 512, fill3, 0)

    def fill4(j, carry):
        col = pl.multiple_of(j * 512, 512)
        acc[:, pl.ds(col, 512)] = partial(0, col)
        return carry

    lax.fori_loop(0, width // 512, fill4, 0)
    stage(1, lines[:1])

    lanes = 128
    el = iota((rows, lanes), 1)
    mt[...] = jnp.zeros((lanes, rows), F32)
    mt[0:2, :] = re_ref[...].astype(F32)
    mt[2:4, :] = sc_ref[...]
    by_token = jnp.transpose(mt[...])
    el_f = el.astype(F32)
    named0 = by_token[:, 0:1] == el_f
    named1 = by_token[:, 1:2] == el_f
    named = jnp.where(named0 | named1, 1.0, 0.0)
    before = jnp.where(iota((rows, rows), 1) < iota((rows, rows), 0), 1.0, 0.0).astype(BF16)
    rank = dot(before, named.astype(BF16))
    slot = jnp.where(named > 0.5, rank, -1.0)
    mtok[...] = slot.astype(BF16)
    mt[...] = jnp.transpose(slot)
    s0 = by_token[:, 2:3]
    s1v = by_token[:, 3:4]
    total = s0 + s1v
    shr[...] = (
        jnp.where(named0, s0 / total, 0.0) + jnp.where(named1, s1v / total, 0.0)
    ).astype(BF16)

    plus1.wait_recv()
    s2[0, 1] = (accp[...] + r1[0].astype(F32)).astype(BF16)
    plus3.start()
    minus1.wait_recv()
    s2[1, 1] = (accm[...] + r1[1].astype(F32)).astype(BF16)
    minus3.start()
    for i, swap in enumerate(swaps):
        weight_copy(i, 0).wait_recv()
        swap.start()
    stage(2, lines[1:2])

    lane16 = lax.rem(iota((rows, lanes), 1), BLK)
    tail_at = 3 * (lane16 - CAP)

    def weights_of(g, carry):
        spread = jnp.where(iota((lanes, lanes), 0) == g * 8 + iota((lanes, lanes), 1) // BLK, 1.0, 0.0)
        spread = spread.astype(BF16)
        at = dot(mtok[...], spread)
        share = dot(shr[...], spread)
        for k in range(4):
            if k < 3:
                want = jnp.where(lane16 >= CAP, tail_at + k, -5)
            else:
                want = jnp.where(lane16 < CAP, lane16, -5)
            onehot[k, g] = jnp.where(at == want.astype(F32), share, 0.0).astype(BF16)
        return carry

    lax.fori_loop(0, NZ, weights_of, 0)

    locals_[2].wait()
    plus2.wait_recv()
    minus2.wait_recv()
    plus3.wait_recv()
    minus3.wait_recv()

    def norm(b, carry):
        at = pl.ds(pl.multiple_of(b * 32, 32), 32)
        halves = []
        for h in range(2):
            cols = pl.ds(h * half, half)
            projected = acc[at, cols] + rl[h, at, :].astype(F32) + rr[h, at, :].astype(F32)
            m = (res[at, cols].astype(F32) + projected).astype(BF16)
            middle[at, cols] = m
            halves.append(m.astype(F32))
        squares = sum(jnp.sum(m * m, axis=1, keepdims=True) for m in halves)
        factor = lax.rsqrt(squares / width + 1e-06)
        for h in range(2):
            cols = pl.ds(h * half, half)
            normed[at, cols] = (halves[h] * factor * gain_ref[:, cols]).astype(BF16)
        return carry

    lax.fori_loop(0, rows // 32, norm, 0)

    def lag_of(g):
        return 4 + ((g + 1) // 2) * (1 - 2 * lax.rem(g, 2))

    gl = 8 * BLK
    row16 = lax.rem(iota((gl, rows), 0), BLK)
    sign = 1 - 2 * c

    def block(idx):
        return pl.ds(pl.multiple_of(idx * BLK, BLK), BLK)

    def place(lag, yy, cc):
        ze = lax.rem(z - lag + NZ, NZ)
        own = lag == 0
        plus = (lag < 4) | ((lag == 4) & (c == 0))
        shift = jnp.where(own, 0, jnp.where(plus, 1, NZ - 1))
        j = jnp.where(plus, lag - 1, 7 - lag)
        away = jnp.where(x // 2 == cc, 0, 1)
        core = jnp.where(own, cc, jnp.where(plus, 0, 1))
        xx = jnp.where(own | (away == 0), x, mirror)
        slot = jnp.where(
            own, y * 2 + c, jnp.where(j < 3, 8 + 16 * j + (y * 2 + c) * 2 + away, 56 + y * 2 + away)
        )
        dev = (lax.rem(ze + shift, NZ), yy, core, xx)
        return (ze * NY + yy) * NC + cc, dev, slot

    def is_me(dev):
        return (dev[0] == z) & (dev[1] == y) & (dev[2] == c) & (dev[3] == x)

    def origin(slot_group, yy, cc, away):
        if slot_group == "own":
            return (z, yy, cc, x), yy * 2 + cc, me
        j = slot_group
        zz = lax.rem(z + sign * j + NZ, NZ)
        xx = jnp.where(away == 0, x, mirror)
        slot = jnp.where(j < 3, 8 + 16 * j + (yy * 2 + cc) * 2 + away, 56 + yy * 2 + away)
        return (zz, yy, cc, xx), slot, imported

    imported = (lax.rem(z - sign + NZ, NZ) * NY + y) * NC + x // 2

    def members(group, act):
        if isinstance(group, str):
            todo = [(q // NC, q % NC, 0) for q in range(8)]
        elif isinstance(group, int):
            todo = [(q, c, away) for q in range(4) for away in range(2)]
        else:
            todo = [(q // NC, q % NC, away) for q in range(8) for away in range(2)]
        for q, cc, away in todo:
            core = cc if isinstance(group, int) else lax.rem(c + cc, NC)
            dev, slot, expert = origin(group, lax.rem(y + q, NY), core, away)
            pl.when(jnp.logical_not(is_me(dev)))(functools.partial(act, dev, slot, expert))

    def out_copy(expert, dev, slot):
        return pltpu.make_async_remote_copy(
            src_ref=send.at[block(expert), :], dst_ref=recv.at[block(slot), :],
            send_sem=d_send.at[expert], recv_sem=d_recv.at[slot],
            device_id=dev, device_id_type=MESH,
        )

    def back_copy(dev, slot, expert):
        return pltpu.make_async_remote_copy(
            src_ref=ret.at[block(slot), :], dst_ref=back.at[block(expert), :],
            send_sem=b_send.at[slot], recv_sem=b_recv.at[expert],
            device_id=dev, device_id_type=MESH,
        )

    def back_wait(expert, dev):
        return pltpu.make_async_remote_copy(
            src_ref=ret.at[block(expert), :], dst_ref=back.at[block(expert), :],
            send_sem=b_send.at[expert], recv_sem=b_recv.at[expert],
            device_id=dev, device_id_type=MESH,
        )

    def each_expert(lag, act):
        for q in range(8):
            expert, dev, slot = place(lag, lax.rem(y + q // NC, NY), lax.rem(c + q % NC, NC))
            pl.when(jnp.logical_not(is_me(dev)))(functools.partial(act, expert, dev, slot))

    def dispatch(g, carry):
        lag = lag_of(g)
        ze = lax.rem(z - lag + NZ, NZ)
        at8 = mt[pl.ds(pl.multiple_of(ze * 8, 8), 8), :]
        at = jnp.broadcast_to(at8[:, None, :], (8, BLK, rows)).reshape(gl, rows)
        main = jnp.where(at == jnp.where(row16 < CAP, row16, -5).astype(F32), 1.0, 0.0).astype(BF16)
        at_rows = pl.ds(pl.multiple_of(ze * gl, gl), gl)
        for k in range(3):
            want = jnp.where(row16 >= CAP, 3 * (row16 - CAP) + k, -5).astype(F32)
            tail = jnp.where(at == want, 1.0, 0.0).astype(BF16)
            cols = pl.ds(k * q4, q4)
            packed = dot(main, normed[:, cols]) + dot(tail, normed[:, pl.ds(3 * q4, q4)])
            send[at_rows, cols] = packed.astype(BF16)
        each_expert(lag, lambda expert, dev, slot: out_copy(expert, dev, slot).start())
        return carry

    lax.fori_loop(0, NZ, dispatch, 0)
    own_slot, far_slot = y * 2 + c, 8 + (y * 2 + c) * 2
    recv[block(own_slot), :] = send[block(me), :]
    recv[block(far_slot), :] = send[block(imported), :]
    for i in (3, 4, 5):
        locals_[i].wait()

    def ffn(group, first, count, gate_w, up_w, down_w):
        members(group, lambda dev, slot, expert: out_copy(slot, dev, slot).wait_recv())
        ra, ca = iota((count, count), 0), iota((count, count), 1)
        same = ra // BLK == ca // BLK
        r16, c16 = lax.rem(ra, BLK), lax.rem(ca, BLK)
        keep = lax.rem(iota((count, q4), 0), BLK) < CAP
        at_rows = pl.ds(pl.multiple_of(first * BLK, 128), count)
        tail = jnp.zeros((count, q4), F32)
        for k in range(3):
            pick = jnp.where(same & (c16 >= CAP) & (r16 == 3 * (c16 - CAP) + k), 1.0, 0.0)
            tail = tail + dot(pick.astype(BF16), recv[at_rows, pl.ds(k * q4, q4)])
        tail = tail.astype(BF16)
        rows_in = recv[at_rows, :]
        gate = dot(rows_in, gate_w[pl.ds(0, 3 * q4), :]) + dot(tail, gate_w[pl.ds(3 * q4, q4), :])
        up = dot(rows_in, up_w[pl.ds(0, 3 * q4), :]) + dot(tail, up_w[pl.ds(3 * q4, q4), :])
        hidden = (gate / (1.0 + jnp.exp(-gate)) * up).astype(BF16)
        last = dot(hidden, down_w[:, pl.ds(3 * q4, q4)]).astype(BF16)
        for k in range(3):
            put = jnp.where(same & (r16 >= CAP) & (c16 == 3 * (r16 - CAP) + k), 1.0, 0.0)
            cols = pl.ds(k * q4, q4)
            ret[at_rows, cols] = jnp.where(
                keep, dot(hidden, down_w[:, cols]), dot(put.astype(BF16), last)
            ).astype(BF16)
        members(group, lambda dev, slot, expert: back_copy(dev, slot, expert).start())

    ffn("own", 0, 8 * BLK, wg, wu, wd)
    back[block(me), :] = ret[block(own_slot), :]
    for i in (2, 3):
        weight_copy(i, 0).wait_recv()
    for swap in swaps:
        swap.wait_recv()

    def far(i, carry):
        j = jnp.where(i == 0, 0, 3 - i)
        ffn(j, 8 + 16 * j, 16 * BLK, wg2, wu2, wd2)
        return carry

    lax.fori_loop(0, 1, far, 0)
    back[block(imported), :] = ret[block(far_slot), :]
    ffn(3, 56, 8 * BLK, wg2, wu2, wd2)
    lax.fori_loop(1, 3, far, 0)

    def clear(b, carry):
        at = pl.ds(pl.multiple_of(b * 32, 32), 32)
        acc[at, :] = middle[at, :].astype(F32)
        return carry

    lax.fori_loop(0, rows // 32, clear, 0)

    def combine(g, carry):
        lag = jnp.where(g < 2, g, jnp.where(g == 2, 7, jnp.where(g == 3, 4, jnp.where(
            g < 6, 2 * g - 5, 4 * g - 22))))
        zz = lax.rem(z - lag + NZ, NZ)
        each_expert(lag, lambda expert, dev, slot: back_wait(expert, dev).wait_recv())
        at_rows = pl.ds(pl.multiple_of(zz * gl, gl), gl)
        extra = acc[:, pl.ds(3 * q4, q4)]
        for k in range(3):
            cols = pl.ds(k * q4, q4)
            piece = back[at_rows, cols]
            acc[:, cols] += dot(onehot[3, zz], piece)
            extra = extra + dot(onehot[k, zz], piece)
        acc[:, pl.ds(3 * q4, q4)] = extra
        return carry

    lax.fori_loop(0, NZ, combine, 0)

    def finish(b, carry):
        at = pl.ds(pl.multiple_of(b * 32, 32), 32)
        out_ref[at, :] = acc[at, :].astype(BF16)
        return carry

    lax.fori_loop(0, rows // 32, finish, 0)
    for cp in (plus1, minus1, plus2, minus2, plus3, minus3):
        cp.wait_send()

    def drain(g, carry):
        each_expert(g, lambda expert, dev, slot: out_copy(expert, dev, slot).wait_send())
        return carry

    lax.fori_loop(0, NZ, drain, 0)
    members("own", lambda dev, slot, expert: back_copy(dev, slot, expert).wait_send())
    members(3, lambda dev, slot, expert: back_copy(dev, slot, expert).wait_send())

    def drain_far(j, carry):
        members(j, lambda dev, slot, expert: back_copy(dev, slot, expert).wait_send())
        return carry

    lax.fori_loop(0, 3, drain_far, 0)

    halo.wait_send()
    for swap in swaps:
        swap.wait_send()

    @pl.when(gives)
    def _():
        for i in range(4):
            for side in range(2):
                weight_copy(i, side).wait_send()


def body(
    pooled_in, group_map, pool_scale, out_weight, residual, norm_gain,
    gate_weight, up_weight, down_weight, route_expert, route_score,
):
    tok, ch = pooled_in.shape
    rows, width = residual.shape
    ff = gate_weight.shape[2]
    half = width // 2
    packed = (NSP * BLK, 3 * width // 4)
    vmem = pl.BlockSpec(memory_space=pltpu.VMEM)
    hbm = pl.BlockSpec(memory_space=pl.ANY)
    dma = pltpu.SemaphoreType.DMA
    return pl.pallas_call(
        kernel,
        out_shape=jax.ShapeDtypeStruct((rows, width), BF16),
        in_specs=[hbm, vmem, vmem, hbm, hbm, vmem, hbm, hbm, hbm, vmem, vmem],
        out_specs=vmem,
        scratch_shapes=[
            pltpu.VMEM((HALO + tok, ch), BF16),
            pltpu.VMEM((ch, width), BF16),
            pltpu.VMEM((rows, width), BF16),
            pltpu.VMEM((width, ff), BF16),
            pltpu.VMEM((width, ff), BF16),
            pltpu.VMEM((ff, width), BF16),
            pltpu.VMEM((width, ff), BF16),
            pltpu.VMEM((width, ff), BF16),
            pltpu.VMEM((ff, width), BF16),
            pltpu.VMEM((tok, ch), BF16),
            pltpu.VMEM((2, rows, half), BF16),
            pltpu.VMEM((2, 2, rows, half), BF16),
            pltpu.VMEM((2, rows, half), BF16),
            pltpu.VMEM((2, rows, half), BF16),
            pltpu.VMEM((2, rows, half), BF16),
            pltpu.VMEM((rows, half), F32),
            pltpu.VMEM((rows, half), F32),
            pltpu.VMEM((rows, width), F32),
            pltpu.VMEM((rows, width), BF16),
            pltpu.VMEM((rows, width), BF16),
            pltpu.VMEM((128, rows), F32),
            pltpu.VMEM((rows, 128), BF16),
            pltpu.VMEM((rows, 128), BF16),
            pltpu.VMEM((4, NZ, rows, 128), BF16),
            pltpu.VMEM(packed, BF16),
            pltpu.VMEM(packed, BF16),
            pltpu.VMEM(packed, BF16),
            pltpu.VMEM(packed, BF16),
            dma((6,)),
            pltpu.SemaphoreType.REGULAR((3,)),
            dma((2,)),
            dma((4,)),
            dma((8,)),
            dma((4,)),
            dma((6,)),
            dma((6,)),
            dma((NSP,)),
            dma((NSP,)),
            dma((NSP,)),
            dma((NSP,)),
        ],
        compiler_params=pltpu.CompilerParams(
            collective_id=0, has_side_effects=True, vmem_limit_bytes=60 * 2**20
        ),
    )(
        pooled_in, group_map, pool_scale.reshape(1, -1), out_weight, residual,
        norm_gain.reshape(1, -1), gate_weight.reshape(width, ff), up_weight.reshape(width, ff),
        down_weight.reshape(ff, width), route_expert.T, route_score.T,
    )


def solution(mesh):
    split = Mesh(mesh.devices.reshape(NZ, NY, NC, NX), AXES)
    sp_tp = AXES
    in_specs = (
        P(SP, "x"),
        P("x", None, None),
        P("x"),
        P("x", None),
        P(sp_tp, None),
        P(),
        P(SP, None, None),
        P(SP, None, None),
        P(SP, None, None),
        P(sp_tp, None),
        P(sp_tp, None),
    )
    return jax.shard_map(
        body, mesh=split, in_specs=in_specs, out_specs=P(sp_tp, None), check_vma=False
    )
```

```python
import functools

import jax
import jax.numpy as jnp
from jax import lax
from jax.experimental import pallas as pl
from jax.experimental.pallas import tpu as pltpu
from jax.sharding import Mesh
from jax.sharding import PartitionSpec as P

AXES = ("z", "y", "c", "x")
SP = ("z", "y", "c")
MESH = pl.DeviceIdType.MESH
NZ, NY, NC, NX = 8, 4, 2, 4
NSP = NZ * NY * NC
HALO = 16
CAP = 12
BLK = 16
F32, BF16 = jnp.float32, jnp.bfloat16


def dot(a, b):
    return jnp.dot(a, b, preferred_element_type=F32)


def iota(shape, dim):
    return lax.broadcasted_iota(jnp.int32, shape, dim)


def kernel(
    pin_hbm, gm_ref, scale_ref, ow_hbm, res_hbm, gain_ref, wg_hbm, wu_hbm, wd_hbm, re_ref, sc_ref,
    out_ref,
    ext, ow, res, wg, wu, wd, wg2, wu2, wd2, pooled,
    s1, s2, r1, rl, rr, accp, accm, acc, middle, normed,
    mt, mtok, shr, onehot,
    send, recv, ret, back,
    lsem, gate_sem, halo_sem, swap_sem, w_send, w_recv, rs_send, rs_recv, d_send, d_recv, b_send, b_recv,
):
    z, y, c, x = (lax.axis_index(a) for a in AXES)
    me = (z * NY + y) * NC + c
    rows = res_hbm.shape[0]
    width = res_hbm.shape[1]
    tok = pin_hbm.shape[0]
    half = width // 2
    q4 = width // 4

    def sp_peer(idx, xx=x):
        return (idx // (NY * NC), (idx // NC) % NY, idx % NC, xx)

    mirror = NX - 1 - x

    def x_peer(d):
        return (z, y, c, lax.rem(x + d, NX))

    barrier = pltpu.get_barrier_semaphore()

    lines = [(z, y, 1 - c, x), (z, y, c, mirror), (z, y, c, x + 1 - 2 * lax.rem(x, 2))]
    y_line = [(z, lax.rem(y + k, NY), c, x) for k in range(1, NY)]
    lines += y_line + [(lax.rem(z + k, NZ), y, c, x) for k in range(1, NZ)]
    lines.append(sp_peer(lax.rem(me + 2 * c - 1 + NSP, NSP)))
    lines += [(lax.rem(z + k, NZ), y, 1 - c, x) for k in (1, NZ - 1)]
    for dev in lines:
        pl.semaphore_signal(barrier, inc=1, device_id=dev, device_id_type=MESH)

    def stage(i, devs):
        for dev in devs:
            pl.semaphore_signal(gate_sem.at[i], inc=1, device_id=dev, device_id_type=MESH)
        pl.semaphore_wait(gate_sem.at[i], len(devs))

    locals_ = [
        pltpu.make_async_copy(src, dst, lsem.at[i])
        for i, (src, dst) in enumerate(
            (
                (pin_hbm, ext.at[pl.ds(HALO, tok), :]),
                (ow_hbm, ow),
                (res_hbm, res),
                (wg_hbm, wg),
                (wu_hbm, wu),
                (wd_hbm, wd),
            )
        )
    ]
    for cp in locals_:
        cp.start()
    pl.semaphore_wait(barrier, len(lines))

    halo = pltpu.make_async_remote_copy(
        src_ref=pin_hbm.at[pl.ds(tok - HALO, HALO), :],
        dst_ref=ext.at[pl.ds(0, HALO), :],
        send_sem=halo_sem.at[0],
        recv_sem=halo_sem.at[1],
        device_id=sp_peer(lax.rem(me + 1, NSP)),
        device_id_type=MESH,
    )
    halo.start()

    gives = c == x // 2

    mid = wd_hbm.shape[0] // 2
    pair = x + 1 - 2 * lax.rem(x, 2)

    share = 7 * wu_hbm.shape[0] // 16
    rest = pl.ds(2 * share, wu_hbm.shape[0] - 2 * share)

    def mine(ref, count):
        return ref.at[pl.ds(pl.multiple_of(lax.rem(x, 2) * count, count), count), :]

    def weight_copy(i, side):
        src = (mine(wd_hbm, mid), mine(wu_hbm, share), wg_hbm, wu_hbm.at[rest, :])[i]
        dst = (mine(wd2, mid), mine(wu2, share), wg2, wu2.at[rest, :])[i]
        return pltpu.make_async_remote_copy(
            src_ref=src, dst_ref=dst, send_sem=w_send.at[2 * i + side], recv_sem=w_recv.at[i],
            device_id=(lax.rem(z + (1, NZ - 1)[side], NZ), y, side, x), device_id_type=MESH,
        )

    swaps = [
        pltpu.make_async_remote_copy(
            src_ref=part, dst_ref=part, send_sem=swap_sem.at[2 * i], recv_sem=swap_sem.at[2 * i + 1],
            device_id=(z, y, c, pair), device_id_type=MESH,
        )
        for i, part in enumerate((mine(wd2, mid), mine(wu2, share)))
    ]

    @pl.when(gives)
    def _():
        for i in range(4):
            for side in range(2):
                weight_copy(i, side).start()

    window = jnp.left_shift(jnp.int32(2), x)
    step = 128
    lag = iota((step, step + HALO), 0) + HALO - iota((step, step + HALO), 1)
    in_band = jnp.where((lag >= 0) & (lag < window), 1.0, 0.0)
    first_col = iota((step, step + HALO), 1) < HALO

    locals_[0].wait()
    pl.when(x == 2)(halo.wait_recv)

    per = rows // step

    def pool(i, carry):
        part = i // per
        d = jnp.where(part == 0, 2, jnp.where(part == 3, 0, 2 * part - 1))
        b = lax.rem(x + d, NX) * per + lax.rem(i, per)
        t0 = pl.multiple_of(b * step, step)
        start_of_all = (me == 0) & (b == 0)
        band = jnp.where(first_col & start_of_all, 0.0, in_band).astype(BF16)
        running = dot(band, ext[pl.ds(t0, step + HALO), :])
        pos = me * tok + t0 + iota((step, 1), 0)
        inverse = 1.0 / jnp.minimum(pos + 1, window).astype(F32)
        own = ext[pl.ds(t0 + HALO, step), :].astype(F32)
        contrast = (running * inverse - own).astype(BF16)
        mixture = dot(contrast, gm_ref[0])
        pooled[pl.ds(t0, step), :] = (mixture * scale_ref[...]).astype(BF16)
        return carry

    lax.fori_loop(0, per, pool, 0)
    locals_[1].wait()

    def partial(d, col):
        base = pl.multiple_of(lax.rem(x + d, NX) * rows, rows)
        return dot(pooled[pl.ds(base, rows), :], ow[:, pl.ds(pl.multiple_of(col, 512), 512)])

    def rs_copy(i, src, dst, d):
        return pltpu.make_async_remote_copy(
            src_ref=src, dst_ref=dst, send_sem=rs_send.at[i], recv_sem=rs_recv.at[i],
            device_id=x_peer(d), device_id_type=MESH,
        )

    lo, hi = pl.ds(0, half), pl.ds(half, half)
    plus1 = rs_copy(0, s1.at[0], r1.at[0], 1)
    minus1 = rs_copy(1, s1.at[1], r1.at[1], NX - 1)
    plus2 = rs_copy(2, s2.at[0, 0], rl.at[1], 1)
    minus2 = rs_copy(3, s2.at[1, 0], rr.at[0], NX - 1)
    plus3 = rs_copy(4, s2.at[0, 1], rl.at[0], 1)
    minus3 = rs_copy(5, s2.at[1, 1], rr.at[1], NX - 1)

    def fill(j, carry):
        col = pl.multiple_of(j * 512, 512)
        s1[0, :, pl.ds(col, 512)] = partial(2, col).astype(BF16)
        s1[1, :, pl.ds(col, 512)] = partial(2, half + col).astype(BF16)
        return carry

    lax.fori_loop(0, half // 512, fill, 0)
    plus1.start()
    minus1.start()
    pl.when(x != 2)(halo.wait_recv)
    lax.fori_loop(per, NX * per, pool, 0)

    def fill2(j, carry):
        col = pl.multiple_of(j * 512, 512)
        s2[0, 0, :, pl.ds(col, 512)] = partial(1, half + col).astype(BF16)
        s2[1, 0, :, pl.ds(col, 512)] = partial(NX - 1, col).astype(BF16)
        return carry

    lax.fori_loop(0, half // 512, fill2, 0)
    plus2.start()
    minus2.start()
    stage(0, y_line)

    def fill3(j, carry):
        col = pl.multiple_of(j * 512, 512)
        accp[:, pl.ds(col, 512)] = partial(1, col)
        accm[:, pl.ds(col, 512)] = partial(NX - 1, half + col)
        return carry

    lax.fori_loop(0, half // 512, fill3, 0)

    def fill4(j, carry):
        col = pl.multiple_of(j * 512, 512)
        acc[:, pl.ds(col, 512)] = partial(0, col)
        return carry

    lax.fori_loop(0, width // 512, fill4, 0)
    stage(1, lines[:1])

    lanes = 128
    el = iota((rows, lanes), 1)
    mt[...] = jnp.zeros((lanes, rows), F32)
    mt[0:2, :] = re_ref[...].astype(F32)
    mt[2:4, :] = sc_ref[...]
    by_token = jnp.transpose(mt[...])
    el_f = el.astype(F32)
    named0 = by_token[:, 0:1] == el_f
    named1 = by_token[:, 1:2] == el_f
    named = jnp.where(named0 | named1, 1.0, 0.0)
    before = jnp.where(iota((rows, rows), 1) < iota((rows, rows), 0), 1.0, 0.0).astype(BF16)
    rank = dot(before, named.astype(BF16))
    slot = jnp.where(named > 0.5, rank, -1.0)
    mtok[...] = slot.astype(BF16)
    mt[...] = jnp.transpose(slot)
    s0 = by_token[:, 2:3]
    s1v = by_token[:, 3:4]
    total = s0 + s1v
    shr[...] = (
        jnp.where(named0, s0 / total, 0.0) + jnp.where(named1, s1v / total, 0.0)
    ).astype(BF16)

    plus1.wait_recv()
    s2[0, 1] = (accp[...] + r1[0].astype(F32)).astype(BF16)
    plus3.start()
    minus1.wait_recv()
    s2[1, 1] = (accm[...] + r1[1].astype(F32)).astype(BF16)
    minus3.start()
    for i, swap in enumerate(swaps):
        weight_copy(i, 0).wait_recv()
        swap.start()
    stage(2, lines[1:2])

    lane16 = lax.rem(iota((rows, lanes), 1), BLK)
    tail_at = 3 * (lane16 - CAP)

    def weights_of(g, carry):
        spread = jnp.where(iota((lanes, lanes), 0) == g * 8 + iota((lanes, lanes), 1) // BLK, 1.0, 0.0)
        spread = spread.astype(BF16)
        at = dot(mtok[...], spread)
        share = dot(shr[...], spread)
        for k in range(4):
            if k < 3:
                want = jnp.where(lane16 >= CAP, tail_at + k, -5)
            else:
                want = jnp.where(lane16 < CAP, lane16, -5)
            onehot[k, g] = jnp.where(at == want.astype(F32), share, 0.0).astype(BF16)
        return carry

    lax.fori_loop(0, NZ, weights_of, 0)

    locals_[2].wait()
    plus2.wait_recv()
    minus2.wait_recv()
    plus3.wait_recv()
    minus3.wait_recv()

    def norm(b, carry):
        at = pl.ds(pl.multiple_of(b * 32, 32), 32)
        halves = []
        for h in range(2):
            cols = pl.ds(h * half, half)
            projected = acc[at, cols] + rl[h, at, :].astype(F32) + rr[h, at, :].astype(F32)
            m = (res[at, cols].astype(F32) + projected).astype(BF16)
            middle[at, cols] = m
            halves.append(m.astype(F32))
        squares = sum(jnp.sum(m * m, axis=1, keepdims=True) for m in halves)
        factor = lax.rsqrt(squares / width + 1e-06)
        for h in range(2):
            cols = pl.ds(h * half, half)
            normed[at, cols] = (halves[h] * factor * gain_ref[:, cols]).astype(BF16)
        return carry

    lax.fori_loop(0, rows // 32, norm, 0)

    def lag_of(g):
        return 4 + ((g + 1) // 2) * (1 - 2 * lax.rem(g, 2))

    gl = 8 * BLK
    row16 = lax.rem(iota((gl, rows), 0), BLK)
    sign = 1 - 2 * c

    def block(idx):
        return pl.ds(pl.multiple_of(idx * BLK, BLK), BLK)

    def place(lag, yy, cc):
        ze = lax.rem(z - lag + NZ, NZ)
        own = lag == 0
        plus = (lag < 4) | ((lag == 4) & (c == 0))
        shift = jnp.where(own, 0, jnp.where(plus, 1, NZ - 1))
        j = jnp.where(plus, lag - 1, 7 - lag)
        away = jnp.where(x // 2 == cc, 0, 1)
        core = jnp.where(own, cc, jnp.where(plus, 0, 1))
        xx = jnp.where(own | (away == 0), x, mirror)
        slot = jnp.where(
            own, y * 2 + c, jnp.where(j < 3, 8 + 16 * j + (y * 2 + c) * 2 + away, 56 + y * 2 + away)
        )
        dev = (lax.rem(ze + shift, NZ), yy, core, xx)
        return (ze * NY + yy) * NC + cc, dev, slot

    def is_me(dev):
        return (dev[0] == z) & (dev[1] == y) & (dev[2] == c) & (dev[3] == x)

    def origin(slot_group, yy, cc, away):
        if slot_group == "own":
            return (z, yy, cc, x), yy * 2 + cc, me
        j = slot_group
        zz = lax.rem(z + sign * j + NZ, NZ)
        xx = jnp.where(away == 0, x, mirror)
        slot = jnp.where(j < 3, 8 + 16 * j + (yy * 2 + cc) * 2 + away, 56 + yy * 2 + away)
        return (zz, yy, cc, xx), slot, imported

    imported = (lax.rem(z - sign + NZ, NZ) * NY + y) * NC + x // 2

    def members(group, act):
        if isinstance(group, str):
            todo = [(q // NC, q % NC, 0) for q in range(8)]
        elif isinstance(group, int):
            todo = [(q, c, away) for q in range(4) for away in range(2)]
        else:
            todo = [(q // NC, q % NC, away) for q in range(8) for away in range(2)]
        for q, cc, away in todo:
            core = cc if isinstance(group, int) else lax.rem(c + cc, NC)
            dev, slot, expert = origin(group, lax.rem(y + q, NY), core, away)
            pl.when(jnp.logical_not(is_me(dev)))(functools.partial(act, dev, slot, expert))

    def out_copy(expert, dev, slot):
        return pltpu.make_async_remote_copy(
            src_ref=send.at[block(expert), :], dst_ref=recv.at[block(slot), :],
            send_sem=d_send.at[expert], recv_sem=d_recv.at[slot],
            device_id=dev, device_id_type=MESH,
        )

    def back_copy(dev, slot, expert):
        return pltpu.make_async_remote_copy(
            src_ref=ret.at[block(slot), :], dst_ref=back.at[block(expert), :],
            send_sem=b_send.at[slot], recv_sem=b_recv.at[expert],
            device_id=dev, device_id_type=MESH,
        )

    def back_wait(expert, dev):
        return pltpu.make_async_remote_copy(
            src_ref=ret.at[block(expert), :], dst_ref=back.at[block(expert), :],
            send_sem=b_send.at[expert], recv_sem=b_recv.at[expert],
            device_id=dev, device_id_type=MESH,
        )

    def each_expert(lag, act):
        for q in range(8):
            expert, dev, slot = place(lag, lax.rem(y + q // NC, NY), lax.rem(c + q % NC, NC))
            pl.when(jnp.logical_not(is_me(dev)))(functools.partial(act, expert, dev, slot))

    def dispatch(g, carry):
        lag = lag_of(g)
        ze = lax.rem(z - lag + NZ, NZ)
        at8 = mt[pl.ds(pl.multiple_of(ze * 8, 8), 8), :]
        at = jnp.broadcast_to(at8[:, None, :], (8, BLK, rows)).reshape(gl, rows)
        main = jnp.where(at == jnp.where(row16 < CAP, row16, -5).astype(F32), 1.0, 0.0).astype(BF16)
        at_rows = pl.ds(pl.multiple_of(ze * gl, gl), gl)
        for k in range(3):
            want = jnp.where(row16 >= CAP, 3 * (row16 - CAP) + k, -5).astype(F32)
            tail = jnp.where(at == want, 1.0, 0.0).astype(BF16)
            cols = pl.ds(k * q4, q4)
            packed = dot(main, normed[:, cols]) + dot(tail, normed[:, pl.ds(3 * q4, q4)])
            send[at_rows, cols] = packed.astype(BF16)
        each_expert(lag, lambda expert, dev, slot: out_copy(expert, dev, slot).start())
        return carry

    lax.fori_loop(0, NZ, dispatch, 0)
    own_slot, far_slot = y * 2 + c, 8 + (y * 2 + c) * 2
    recv[block(own_slot), :] = send[block(me), :]
    recv[block(far_slot), :] = send[block(imported), :]
    for i in (3, 4, 5):
        locals_[i].wait()

    def ffn(group, first, count, gate_w, up_w, down_w):
        members(group, lambda dev, slot, expert: out_copy(slot, dev, slot).wait_recv())
        ra, ca = iota((count, count), 0), iota((count, count), 1)
        same = ra // BLK == ca // BLK
        r16, c16 = lax.rem(ra, BLK), lax.rem(ca, BLK)
        keep = lax.rem(iota((count, q4), 0), BLK) < CAP
        at_rows = pl.ds(pl.multiple_of(first * BLK, 128), count)
        tail = jnp.zeros((count, q4), F32)
        for k in range(3):
            pick = jnp.where(same & (c16 >= CAP) & (r16 == 3 * (c16 - CAP) + k), 1.0, 0.0)
            tail = tail + dot(pick.astype(BF16), recv[at_rows, pl.ds(k * q4, q4)])
        tail = tail.astype(BF16)
        rows_in = recv[at_rows, :]
        gate = dot(rows_in, gate_w[pl.ds(0, 3 * q4), :]) + dot(tail, gate_w[pl.ds(3 * q4, q4), :])
        up = dot(rows_in, up_w[pl.ds(0, 3 * q4), :]) + dot(tail, up_w[pl.ds(3 * q4, q4), :])
        hidden = (gate / (1.0 + jnp.exp(-gate)) * up).astype(BF16)
        last = dot(hidden, down_w[:, pl.ds(3 * q4, q4)]).astype(BF16)
        for k in range(3):
            put = jnp.where(same & (r16 >= CAP) & (c16 == 3 * (r16 - CAP) + k), 1.0, 0.0)
            cols = pl.ds(k * q4, q4)
            ret[at_rows, cols] = jnp.where(
                keep, dot(hidden, down_w[:, cols]), dot(put.astype(BF16), last)
            ).astype(BF16)
        members(group, lambda dev, slot, expert: back_copy(dev, slot, expert).start())

    ffn("own", 0, 8 * BLK, wg, wu, wd)
    back[block(me), :] = ret[block(own_slot), :]
    for i in (2, 3):
        weight_copy(i, 0).wait_recv()
    for swap in swaps:
        swap.wait_recv()

    def far(i, carry):
        j = jnp.where(i == 0, 0, 3 - i)
        ffn(j, 8 + 16 * j, 16 * BLK, wg2, wu2, wd2)
        return carry

    lax.fori_loop(0, 1, far, 0)
    back[block(imported), :] = ret[block(far_slot), :]
    ffn(3, 56, 8 * BLK, wg2, wu2, wd2)
    lax.fori_loop(1, 3, far, 0)

    def clear(b, carry):
        at = pl.ds(pl.multiple_of(b * 32, 32), 32)
        acc[at, :] = middle[at, :].astype(F32)
        return carry

    lax.fori_loop(0, rows // 32, clear, 0)

    def combine(g, carry):
        lag = jnp.where(g < 2, g, jnp.where(g == 2, 7, jnp.where(g == 3, 4, jnp.where(
            g < 6, 2 * g - 5, 4 * g - 22))))
        zz = lax.rem(z - lag + NZ, NZ)
        each_expert(lag, lambda expert, dev, slot: back_wait(expert, dev).wait_recv())
        at_rows = pl.ds(pl.multiple_of(zz * gl, gl), gl)
        extra = acc[:, pl.ds(3 * q4, q4)]
        for k in range(3):
            cols = pl.ds(k * q4, q4)
            piece = back[at_rows, cols]
            acc[:, cols] += dot(onehot[3, zz], piece)
            extra = extra + dot(onehot[k, zz], piece)
        acc[:, pl.ds(3 * q4, q4)] = extra
        return carry

    lax.fori_loop(0, NZ, combine, 0)

    def finish(b, carry):
        at = pl.ds(pl.multiple_of(b * 32, 32), 32)
        out_ref[at, :] = acc[at, :].astype(BF16)
        return carry

    lax.fori_loop(0, rows // 32, finish, 0)
    for cp in (plus1, minus1, plus2, minus2, plus3, minus3):
        cp.wait_send()

    def drain(g, carry):
        each_expert(g, lambda expert, dev, slot: out_copy(expert, dev, slot).wait_send())
        return carry

    lax.fori_loop(0, NZ, drain, 0)
    members("own", lambda dev, slot, expert: back_copy(dev, slot, expert).wait_send())
    members(3, lambda dev, slot, expert: back_copy(dev, slot, expert).wait_send())

    def drain_far(j, carry):
        members(j, lambda dev, slot, expert: back_copy(dev, slot, expert).wait_send())
        return carry

    lax.fori_loop(0, 3, drain_far, 0)

    halo.wait_send()
    for swap in swaps:
        swap.wait_send()

    @pl.when(gives)
    def _():
        for i in range(4):
            for side in range(2):
                weight_copy(i, side).wait_send()


def body(
    pooled_in, group_map, pool_scale, out_weight, residual, norm_gain,
    gate_weight, up_weight, down_weight, route_expert, route_score,
):
    tok, ch = pooled_in.shape
    rows, width = residual.shape
    ff = gate_weight.shape[2]
    half = width // 2
    packed = (NSP * BLK, 3 * width // 4)
    vmem = pl.BlockSpec(memory_space=pltpu.VMEM)
    hbm = pl.BlockSpec(memory_space=pl.ANY)
    dma = pltpu.SemaphoreType.DMA
    return pl.pallas_call(
        kernel,
        out_shape=jax.ShapeDtypeStruct((rows, width), BF16),
        in_specs=[hbm, vmem, vmem, hbm, hbm, vmem, hbm, hbm, hbm, vmem, vmem],
        out_specs=vmem,
        scratch_shapes=[
            pltpu.VMEM((HALO + tok, ch), BF16),
            pltpu.VMEM((ch, width), BF16),
            pltpu.VMEM((rows, width), BF16),
            pltpu.VMEM((width, ff), BF16),
            pltpu.VMEM((width, ff), BF16),
            pltpu.VMEM((ff, width), BF16),
            pltpu.VMEM((width, ff), BF16),
            pltpu.VMEM((width, ff), BF16),
            pltpu.VMEM((ff, width), BF16),
            pltpu.VMEM((tok, ch), BF16),
            pltpu.VMEM((2, rows, half), BF16),
            pltpu.VMEM((2, 2, rows, half), BF16),
            pltpu.VMEM((2, rows, half), BF16),
            pltpu.VMEM((2, rows, half), BF16),
            pltpu.VMEM((2, rows, half), BF16),
            pltpu.VMEM((rows, half), F32),
            pltpu.VMEM((rows, half), F32),
            pltpu.VMEM((rows, width), F32),
            pltpu.VMEM((rows, width), BF16),
            pltpu.VMEM((rows, width), BF16),
            pltpu.VMEM((128, rows), F32),
            pltpu.VMEM((rows, 128), BF16),
            pltpu.VMEM((rows, 128), BF16),
            pltpu.VMEM((4, NZ, rows, 128), BF16),
            pltpu.VMEM(packed, BF16),
            pltpu.VMEM(packed, BF16),
            pltpu.VMEM(packed, BF16),
            pltpu.VMEM(packed, BF16),
            dma((6,)),
            pltpu.SemaphoreType.REGULAR((3,)),
            dma((2,)),
            dma((4,)),
            dma((8,)),
            dma((4,)),
            dma((6,)),
            dma((6,)),
            dma((NSP,)),
            dma((NSP,)),
            dma((NSP,)),
            dma((NSP,)),
        ],
        compiler_params=pltpu.CompilerParams(
            collective_id=0, has_side_effects=True, vmem_limit_bytes=60 * 2**20
        ),
    )(
        pooled_in, group_map, pool_scale.reshape(1, -1), out_weight, residual,
        norm_gain.reshape(1, -1), gate_weight.reshape(width, ff), up_weight.reshape(width, ff),
        down_weight.reshape(ff, width), route_expert.T, route_score.T,
    )


def solution(mesh):
    split = Mesh(mesh.devices.reshape(NZ, NY, NC, NX), AXES)
    sp_tp = AXES
    in_specs = (
        P(SP, "x"),
        P("x", None, None),
        P("x"),
        P("x", None),
        P(sp_tp, None),
        P(),
        P(SP, None, None),
        P(SP, None, None),
        P(SP, None, None),
        P(sp_tp, None),
        P(sp_tp, None),
    )
    return jax.shard_map(
        body, mesh=split, in_specs=in_specs, out_specs=P(sp_tp, None), check_vma=False
    )
```
